512 devices in a mesh: grp: 2 (over y), sp: 32 (over z), tp: 8 (over x, core).
Axes of the slice: x: 4, y: 2, z: 32, core: 2. Of those that a mesh axis runs over, the one named last changes fastest.
The devices are a block of a 4x8x32 slice.
Arguments:
- tokens: bfloat16 [8, 8192, 2048], P('grp', 'sp'), parts along dimension 0, may hold values from -6 to 6
- norm_gain: bfloat16 [2048], replicated, may hold values from 0.099609375 to 1.8984375
- key_weight: bfloat16 [2048, 2048], P(None, 'tp'), may hold values from -0.125 to 0.125
- value_weight: bfloat16 [2048, 2048], P(None, 'tp'), may hold values from -0.125 to 0.125
- break_bias: bfloat16 [8, 8192, 16], P('grp', 'sp', 'tp'), parts along dimension 0, may hold values from -12 to 0
- new_query: bfloat16 [8, 2048], P('grp', 'tp'), parts along dimension 0, may hold values from -6 to 6
Outputs:
- cache_pair: bfloat16 [64, 32, 32, 2, 2048], P(('grp', 'sp'), None, None, None, 'tp'), parts along dimension 0
- cache_bias: bfloat16 [64, 32, 32, 16], P(('grp', 'sp'), None, None, 'tp'), parts along dimension 0
- attended: float32 [8, 2048], P('grp', 'tp'), parts along dimension 0
The draws below stay inside these ranges and needn't reach their ends.
There are 2 independent parts, one for each index of `grp`. The reference program is written for one: setup_inputs(seed, part) draws one part's arguments, and reference() takes and returns one part's arrays. A program takes and returns all parts, laid end to end along the dimension named above; an argument that names none is the same for every part. Nothing has to cross between parts.
All inputs are finite; a program needn't handle non-finite values.
Results may differ from the reference program's by a relative error of at most 0.0064.
Values may be sent and summed in bfloat16 or wider, within the bound.
A program may use at most 64 MiB of HBM per device.

```python
import jax
import jax.numpy as jnp
from jax import lax

D = 2048
HEADS = 16
DH = 128
SEQS = 4
PROMPT_LENGTH = 8192
SPAN = 8
PIECE = 32
N_SP = 32


def draw_break_bias(key, part):
    key_sequence = jax.random.split(key, 6)
    complete_shape = (SEQS, PROMPT_LENGTH, HEADS)
    kind_draw = jax.random.uniform(key_sequence[0], (SEQS, 1, HEADS))
    fast_share = 0.5
    slow_rate = jnp.exp(jax.random.uniform(key_sequence[1], (SEQS, 1, HEADS), minval=jnp.log(0.3), maxval=jnp.log(0.8))) / PROMPT_LENGTH
    fast_rate = jnp.exp(jax.random.uniform(key_sequence[2], (SEQS, 1, HEADS), minval=jnp.log(0.01), maxval=jnp.log(1.0 / 30.0)))
    decay_rate = jnp.where(kind_draw < fast_share, fast_rate, slow_rate)
    block_multiplier = jax.random.uniform(key_sequence[3], (SEQS, 32, 1, HEADS), minval=-0.7, maxval=0.7)
    block_multiplier = jnp.broadcast_to(block_multiplier, (SEQS, 32, PROMPT_LENGTH // 32, HEADS)).reshape(complete_shape)
    constant_level = jnp.log(decay_rate) + block_multiplier
    spike_marker = jax.random.uniform(key_sequence[4], complete_shape) < 4.0 / PROMPT_LENGTH
    spike_threshold = jax.random.uniform(key_sequence[5], complete_shape, minval=-1.4, maxval=0.0)
    return jnp.where(spike_marker, spike_threshold, constant_level).astype(jnp.bfloat16)


def level_of(rng, shape, shards, least, top_value):
    loudness = 1.0
    for axis_at, parts in shards:
        draws = jax.random.uniform(jax.random.fold_in(jax.random.fold_in(rng, 6), axis_at), (parts,), jnp.float32, least / len(shards), top_value / len(shards))
        loudness = loudness * jnp.repeat(jnp.exp(draws), shape[axis_at] // parts).reshape((-1,) + (1,) * (len(shape) - 1 - axis_at))
    return loudness


def centred(rng, shape, scale, most, cuts=(), dtype=jnp.bfloat16):
    array = scale * jax.random.normal(rng, shape, jnp.float32)
    if cuts:
        array = array * level_of(rng, shape, cuts, -0.22, 0.18)
    return jnp.clip(array, -most, most).astype(dtype)


def setup_inputs(seed: int = 0, part: int = 0) -> dict:
    keys = jax.random.split(jax.random.key(seed), 7)
    own_keys = jax.random.split(jax.random.fold_in(keys[6], part), 7)
    return {
        "tokens": centred(own_keys[0], (SEQS, PROMPT_LENGTH, D), 1.0, 6.0, ((1, 32),)),
        "norm_gain": jnp.clip(1.0 + 0.18 * jax.random.normal(keys[1], (D,), jnp.float32), 0.099609375, 1.8984375).astype(jnp.bfloat16),
        "key_weight": centred(keys[2], (D, HEADS * DH), D ** -0.5, 0.125, ((1, 8),)),
        "value_weight": centred(keys[3], (D, HEADS * DH), D ** -0.5, 0.125, ((1, 8),)),
        "break_bias": draw_break_bias(jax.random.fold_in(jax.random.fold_in(keys[6], part), 71), part),
        "new_query": centred(own_keys[5], (SEQS, HEADS * DH), 1.0, 6.0, ((1, 8),)),
    }


norm_eps = 1e-06

def arrange(rows, width):
    shaped = rows.reshape(SEQS, N_SP, SPAN, PIECE, width)
    shaped = jnp.transpose(shaped, (0, 2, 1, 3, 4))
    return shaped.reshape(SEQS * SPAN, N_SP, PIECE, width)

def reference(tokens, norm_gain, key_weight, value_weight, break_bias, new_query):
    widened = tokens.astype(jnp.float32)
    inverse = lax.rsqrt(lax.optimization_barrier(jnp.mean(widened * widened, axis=-1, keepdims=True)) + norm_eps)
    normed = (widened * inverse * norm_gain.astype(jnp.float32)).astype(jnp.bfloat16)
    flat_rows = normed.reshape(SEQS * PROMPT_LENGTH, D)
    key_rows = jnp.dot(flat_rows, key_weight, preferred_element_type=jnp.float32).astype(jnp.bfloat16)
    value_rows = jnp.dot(flat_rows, value_weight, preferred_element_type=jnp.float32).astype(jnp.bfloat16)
    key_rows = key_rows.reshape(SEQS, PROMPT_LENGTH, HEADS * DH)
    value_rows = value_rows.reshape(SEQS, PROMPT_LENGTH, HEADS * DH)
    cache_pair = jnp.stack((arrange(key_rows, HEADS * DH), arrange(value_rows, HEADS * DH)), axis=3)
    cache_bias = arrange(break_bias, HEADS)
    queries = new_query.reshape(SEQS, HEADS, DH).astype(jnp.float32)
    key_heads = key_rows.reshape(SEQS, PROMPT_LENGTH, HEADS, DH).astype(jnp.float32)
    value_heads = value_rows.reshape(SEQS, PROMPT_LENGTH, HEADS, DH).astype(jnp.float32)
    logits = jnp.einsum('shd,sphd->sph', queries, key_heads)
    logits = logits * DH ** (-0.5) + break_bias.astype(jnp.float32)
    keep_log = jax.nn.log_sigmoid(-logits)
    later_sum = lax.cumsum(keep_log, axis=1, reverse=True) - keep_log
    stick_weights = jnp.exp(jax.nn.log_sigmoid(logits) + later_sum).astype(jnp.bfloat16)
    attended = jnp.einsum('sph,sphd->shd', stick_weights.astype(jnp.float32), value_heads)
    return (cache_pair, cache_bias, attended.reshape(SEQS, HEADS * DH))
```

```python
import functools

import jax
import jax.numpy as jnp
from jax import lax
from jax.experimental import pallas as pl
from jax.experimental.pallas import tpu as pltpu
from jax.sharding import PartitionSpec as P

norm_eps = 1e-06
LANES = 128
MESH = pl.DeviceIdType.MESH
F32 = jnp.float32
BF16 = jnp.bfloat16
Z_LAG, X_LAG, P_LAG = 3, 4, 5
READ_AT = 3


def iota(shape, axis):
    return lax.broadcasted_iota(jnp.int32, shape, axis)


def stick(rows, blocks, seqs_heads):
    carry = jnp.zeros((1, LANES), F32)
    carries = [carry]
    for row in rows[:0:-1]:
        carry = carry + row[:, blocks * LANES :]
        carries.append(carry)
    total = carry + rows[0][:, blocks * LANES :]
    factors = jnp.exp(jnp.concatenate(carries[::-1], axis=0))
    stacked = jnp.concatenate([row[:, : blocks * LANES] for row in rows], axis=0)
    parts = []
    for block in range(blocks):
        mine = stacked[:, block * LANES : (block + 1) * LANES] * factors[:, block : block + 1]
        parts.append(jnp.sum(mine, axis=0, keepdims=True))
    return jnp.concatenate(parts, axis=1), total


def kernel(
    shape,
    tokens,
    gain,
    key_weight,
    value_weight,
    bias,
    query,
    cache_out,
    bias_out,
    att_out,
    tok_v,
    weight_v,
    recv,
    normed,
    bias_v,
    bias_recv,
    query_v,
    query_f,
    gain_v,
    gain_f,
    perm,
    later_mask,
    first,
    second,
    load_sem,
    own_sem,
    bias_own_sem,
    z_send,
    z_recv,
    b_send,
    b_recv,
    x_send,
    x_recv,
    p_send,
    p_recv,
    first_send,
    first_recv,
    second_send,
    second_recv,
):
    n, cores, n_x, piece, seqs, heads, width, columns = shape
    steps = n // 2
    span = n // seqs
    rows = span * piece
    feat = width // (cores * n_x)
    head_size = columns // heads
    blocks = seqs * heads
    per_tile = LANES // piece
    z = lax.axis_index("sp")
    tp = lax.axis_index("tp")
    core = lax.rem(tp, cores)
    x = lax.div(tp, cores)
    partner = x * cores + (1 - core)
    mine = pl.ds(pl.multiple_of(tp * feat, feat), feat)

    barrier = pltpu.get_barrier_semaphore()

    def greet(offset, carry):
        pl.semaphore_signal(barrier, 1, device_id={"sp": lax.rem(z + offset, n)}, device_id_type=MESH)
        return carry

    lax.fori_loop(1, n, greet, 0)
    for offset in range(1, n_x):
        pl.semaphore_signal(
            barrier, 1, device_id={"tp": lax.rem(x + offset, n_x) * cores + core}, device_id_type=MESH
        )
    pl.semaphore_signal(barrier, 1, device_id={"tp": partner}, device_id_type=MESH)

    loads = [
        pltpu.make_async_copy(gain, gain_v, load_sem.at[0]),
        pltpu.make_async_copy(bias, bias_v, load_sem.at[1]),
        pltpu.make_async_copy(query, query_v, load_sem.at[2]),
        pltpu.make_async_copy(tokens, tok_v, load_sem.at[3]),
        pltpu.make_async_copy(key_weight, weight_v.at[:, pl.ds(0, columns)], load_sem.at[4]),
        pltpu.make_async_copy(value_weight, weight_v.at[:, pl.ds(columns, columns)], load_sem.at[5]),
    ]
    for load in loads:
        load.start()
    own = pltpu.make_async_copy(
        tokens.at[z, :, mine], recv.at[steps - 1, core, x, pl.ds(piece, piece)], own_sem
    )
    own.start()

    out_row, in_row = iota((4 * 2 * piece, 4 * 2 * piece), 0), iota((4 * 2 * piece, 4 * 2 * piece), 1)
    source = (
        lax.rem(out_row, 2) * (4 * piece)
        + lax.rem(lax.div(out_row, 2), 2) * (2 * piece)
        + lax.div(out_row, 4)
    )
    perm[...] = jnp.where(in_row == source, 1.0, 0.0).astype(BF16)
    later_mask[...] = jnp.where(iota((rows, rows), 0) > iota((rows, rows), 1), 1.0, 0.0).astype(BF16)

    for load in loads[:3]:
        load.wait()
    gains = gain_v[...].astype(F32)
    for t in range(cores * n_x):
        gain_f[t] = jnp.concatenate(
            [gains[t * feat // LANES + j : t * feat // LANES + j + 1] for j in range(feat // LANES)], axis=1
        )
    queries = query_v[...].astype(F32)
    for s in range(seqs):
        query_f[s] = queries[s : s + 1]
    for load in loads[3:]:
        load.wait()

    def project(piece_of, count):
        squares = jnp.zeros((count, feat), F32)
        for t in range(cores * n_x):
            value = piece_of(t).astype(F32)
            squares = squares + value * value
        inverse = lax.rsqrt(jnp.sum(squares, axis=1, keepdims=True) / width + norm_eps)
        for t in range(cores * n_x):
            value = piece_of(t).astype(F32) * inverse * gain_f[t]
            normed[pl.ds(0, count), pl.ds(t * feat, feat)] = value.astype(BF16)
        return jnp.dot(normed[pl.ds(0, count), :], weight_v[...], preferred_element_type=F32).astype(BF16)

    lane = iota((1, LANES), 1)

    def own_read(s, totals):
        projected = project(
            lambda t: tok_v[pl.ds(s * span, span), :, pl.ds(t * feat, feat)].reshape(rows, feat), rows
        )
        keys, values = projected[:, :columns], projected[:, columns:]
        head_row, head_lane = iota((8, columns), 0), lax.div(iota((8, columns), 1), head_size)
        spread = jnp.where(head_row == head_lane, query_f[s], 0.0).astype(BF16)
        logits = lax.dot_general(spread, keys, (((1,), (1,)), ((), ())), preferred_element_type=F32)
        terms = jnp.concatenate([bias_v[s].astype(F32), jnp.zeros((8 - heads, rows), F32)], axis=0)
        logits = logits * head_size ** (-0.5) + terms
        soft = jnp.log1p(jnp.exp(-jnp.abs(logits)))
        keep = jnp.minimum(-logits, 0.0) - soft
        take = jnp.minimum(logits, 0.0) - soft
        high = keep.astype(BF16).astype(F32)
        middle = (keep - high).astype(BF16).astype(F32)
        low = keep - high - middle
        split = jnp.concatenate([high, middle, low, jnp.zeros_like(low)], axis=0).astype(BF16)
        sums = jnp.dot(split, later_mask[...], preferred_element_type=F32)
        later = sums[0:8] + sums[8:16] + sums[16:24]
        weights = jnp.exp(take + later)
        high = weights.astype(BF16).astype(F32)
        split = jnp.concatenate([high, weights - high], axis=0).astype(BF16)
        mixed = jnp.dot(split, values, preferred_element_type=F32)
        mixed = mixed[0:8] + mixed[8:16]
        read = jnp.sum(jnp.where(head_row == head_lane, mixed, 0.0), axis=0, keepdims=True)
        first[lax.rem(z, span), :, pl.ds(pl.multiple_of(s * columns, columns), columns)] = read
        total = jnp.sum(keep, axis=1, keepdims=True)
        for h in range(heads):
            totals = totals + jnp.where(lane == s * heads + h, total[h : h + 1], 0.0)
        return totals

    totals = lax.fori_loop(0, seqs, own_read, jnp.zeros((1, LANES), F32))
    place = lax.rem(z, span)
    group = lax.div(z, span)
    first[place, :, pl.ds(blocks * LANES, LANES)] = totals

    pl.semaphore_wait(barrier, n - 1 + n_x - 1 + 1)

    def first_copy(offset):
        to = group * span + lax.rem(place + offset, span)
        return pltpu.make_async_remote_copy(
            first.at[place], first.at[place], first_send.at[offset - 1], first_recv.at[offset - 1],
            device_id={"sp": to}, device_id_type=MESH,
        )

    def second_copy(offset):
        to = lax.rem(group + offset, seqs) * span + place
        return pltpu.make_async_remote_copy(
            second.at[group], second.at[group], second_send.at[offset - 1], second_recv.at[offset - 1],
            device_id={"sp": to}, device_id_type=MESH,
        )

    for offset in range(1, span):
        first_copy(offset).start()

    def distance(k):
        return steps - k

    def z_copy(k, half):
        to = lax.rem(z + (distance(k) if half == 0 else n - distance(k)), n)
        slot = distance(k) - 1
        return pltpu.make_async_remote_copy(
            tok_v.at[to, :, mine],
            recv.at[slot, core, x, pl.ds(half * piece, piece)],
            z_send.at[slot, half],
            z_recv.at[slot, half],
            device_id={"sp": to},
            device_id_type=MESH,
        )

    def bias_copy(k, half):
        to = lax.rem(z + (distance(k) if half == 0 else n - distance(k)), n)
        tile = lax.div(lax.rem(to, span), per_tile)
        return pltpu.make_async_remote_copy(
            bias_v.at[lax.div(to, span), :, pl.ds(pl.multiple_of(tile * LANES, LANES), LANES)],
            bias_recv.at[z],
            b_send,
            b_recv,
            device_id={"sp": to},
            device_id_type=MESH,
        )

    def x_copy(k, offset):
        slot = distance(k) - 1
        to = lax.rem(x + offset, n_x) * cores + core
        return pltpu.make_async_remote_copy(
            recv.at[slot, core, x],
            recv.at[slot, core, x],
            x_send.at[slot, offset - 1],
            x_recv.at[slot, offset - 1],
            device_id={"tp": to},
            device_id_type=MESH,
        )

    def p_copy(k):
        slot = distance(k) - 1
        return pltpu.make_async_remote_copy(
            recv.at[slot, core], recv.at[slot, core], p_send.at[slot], p_recv.at[slot],
            device_id={"tp": partner}, device_id_type=MESH,
        )

    own_tile = lax.div(lax.rem(z, span), per_tile)
    own_bias = pltpu.make_async_copy(
        bias.at[lax.div(z, span), :, pl.ds(pl.multiple_of(own_tile * LANES, LANES), LANES)],
        bias_recv.at[z],
        bias_own_sem,
    )
    own_bias.start()
    own.wait()

    def step(k, carry):
        @pl.when(k < steps)
        def _():
            z_copy(k, 0).start()
            bias_copy(k, 0).start()

            @pl.when(distance(k) < steps)
            def _():
                z_copy(k, 1).start()
                bias_copy(k, 1).start()

        @pl.when((k >= Z_LAG) & (k < steps + Z_LAG))
        def _():
            z_copy(k - Z_LAG, 0).wait_recv()

            @pl.when(distance(k - Z_LAG) < steps)
            def _():
                z_copy(k - Z_LAG, 1).wait_recv()

            for offset in range(1, n_x):
                x_copy(k - Z_LAG, offset).start()

        @pl.when((k >= X_LAG) & (k < steps + X_LAG))
        def _():
            for offset in range(1, n_x):
                x_copy(k - X_LAG, offset).wait_recv()
            p_copy(k - X_LAG).start()

        @pl.when(k >= P_LAG)
        def _():
            p_copy(k - P_LAG).wait_recv()
            slot = distance(k - P_LAG) - 1
            projected = project(lambda t: recv[slot, t % cores, t // cores], 2 * piece)
            stacked = jnp.concatenate(
                [projected[:, j * LANES : (j + 1) * LANES] for j in range(2 * columns // LANES)], axis=0
            )
            placed = jnp.dot(perm[...], stacked, preferred_element_type=F32).astype(BF16)
            before = lax.rem(z + n - (slot + 1), n)
            after = lax.rem(z + lax.rem(slot + 1, steps), n)
            for half, at in enumerate((before, after)):
                cache_out[pl.ds(pl.multiple_of(at * 4 * piece, 4 * piece), 4 * piece)] = placed[
                    half * 4 * piece : (half + 1) * 4 * piece
                ]

        @pl.when(k == READ_AT)
        def _():
            for offset in range(1, span):
                first_copy(offset).wait_recv()
            read, total = stick([first[j] for j in range(span)], blocks, seqs)
            second[group, :, pl.ds(0, blocks * LANES)] = read
            second[group, :, pl.ds(blocks * LANES, LANES)] = total
            for offset in range(1, seqs):
                second_copy(offset).start()

        return carry

    lax.fori_loop(0, steps + P_LAG, step, 0)

    for offset in range(1, seqs):
        second_copy(offset).wait_recv()
    read, _ = stick([second[j] for j in range(seqs)], blocks, seqs)
    for s in range(seqs):
        att_out[pl.ds(s, 1), :] = read[:, s * columns : (s + 1) * columns]

    own_bias.wait()
    others = pl.ds(0, n - 1)
    pltpu.make_async_copy(bias_recv.at[others], bias_recv.at[others], b_recv).wait()
    arrived = bias_recv[...].astype(F32)
    part = lax.rem(lax.rem(z, span), per_tile)
    chosen = arrived[:, :, 0:piece]
    for j in range(1, per_tile):
        chosen = jnp.where(part == j, arrived[:, :, j * piece : (j + 1) * piece], chosen)
    bias_out[...] = chosen.astype(BF16)

    pltpu.make_async_copy(bias_recv.at[others], bias_recv.at[others], b_send).wait()
    for offset in range(1, span):
        first_copy(offset).wait_send()
    for offset in range(1, seqs):
        second_copy(offset).wait_send()

    def drain(k, carry):
        z_copy(k, 0).wait_send()

        @pl.when(distance(k) < steps)
        def _():
            z_copy(k, 1).wait_send()

        for offset in range(1, n_x):
            x_copy(k, offset).wait_send()
        p_copy(k).wait_send()
        return carry

    lax.fori_loop(0, steps, drain, 0)


def local(cores, tokens, norm_gain, key_weight, value_weight, break_bias, new_query):
    seqs, tok_rows, width = tokens.shape
    heads = break_bias.shape[2]
    columns = key_weight.shape[1]
    n = lax.axis_size("sp")
    n_tp = lax.axis_size("tp")
    n_x = n_tp // cores
    piece = tok_rows * seqs // n
    span = n // seqs
    steps = n // 2
    feat = width // n_tp
    shape = (n, cores, n_x, piece, seqs, heads, width, columns)
    dma = pltpu.SemaphoreType.DMA
    message = seqs * columns + LANES
    cache, bias_out, attended = pl.pallas_call(
        functools.partial(kernel, shape),
        out_shape=(
            jax.ShapeDtypeStruct((n * piece * 4, LANES), BF16),
            jax.ShapeDtypeStruct((n, heads, piece), BF16),
            jax.ShapeDtypeStruct((seqs, columns), F32),
        ),
        in_specs=[pl.BlockSpec(memory_space=pltpu.HBM)] * 6,
        out_specs=[pl.BlockSpec(memory_space=pltpu.VMEM)] * 3,
        scratch_shapes=[
            pltpu.VMEM((n, piece, width), BF16),
            pltpu.VMEM((width, 2 * columns), BF16),
            pltpu.VMEM((steps, cores, n_x, 2 * piece, feat), BF16),
            pltpu.VMEM((max(span, 2) * piece, width), BF16),
            pltpu.VMEM((seqs, heads, tok_rows), BF16),
            pltpu.VMEM((n, heads, LANES), BF16),
            pltpu.VMEM((seqs, columns), BF16),
            pltpu.VMEM((seqs, 1, columns), F32),
            pltpu.VMEM((width // LANES, LANES), BF16),
            pltpu.VMEM((n_tp, 1, feat), F32),
            pltpu.VMEM((8 * piece, 8 * piece), BF16),
            pltpu.VMEM((tok_rows, tok_rows), BF16),
            pltpu.VMEM((span, 1, message), F32),
            pltpu.VMEM((seqs, 1, message), F32),
            dma((6,)),
            dma,
            dma,
            dma((steps, 2)),
            dma((steps, 2)),
            dma,
            dma,
            dma((steps, n_x - 1)),
            dma((steps, n_x - 1)),
            dma((steps,)),
            dma((steps,)),
            dma((span - 1,)),
            dma((span - 1,)),
            dma((seqs - 1,)),
            dma((seqs - 1,)),
        ],
        compiler_params=pltpu.CompilerParams(
            collective_id=0, has_side_effects=True, vmem_limit_bytes=61000000
        ),
    )(
        tokens.reshape(n, piece, width),
        norm_gain.reshape(width // LANES, LANES),
        key_weight,
        value_weight,
        jnp.transpose(break_bias, (0, 2, 1)),
        new_query,
    )
    halves = columns // LANES
    paired = cache.reshape(n, piece, halves, 2, LANES)
    paired = jnp.transpose(paired, (0, 1, 3, 2, 4)).reshape(n, piece, 2, columns)
    return (paired[None], jnp.transpose(bias_out, (0, 2, 1))[None], attended)


def solution(mesh):
    return jax.shard_map(
        functools.partial(local, 2),
        mesh=mesh,
        in_specs=(
            P("grp", "sp", None),
            P(),
            P(None, "tp"),
            P(None, "tp"),
            P("grp", "sp", "tp"),
            P("grp", "tp"),
        ),
        out_specs=(
            P(("grp", "sp"), None, None, None, "tp"),
            P(("grp", "sp"), None, None, "tp"),
            P("grp", "tp"),
        ),
        check_vma=False,
    )
```

```python
import functools

import jax
import jax.numpy as jnp
from jax import lax
from jax.experimental import pallas as pl
from jax.experimental.pallas import tpu as pltpu
from jax.sharding import PartitionSpec as P

norm_eps = 1e-06
LANES = 128
MESH = pl.DeviceIdType.MESH
F32 = jnp.float32
BF16 = jnp.bfloat16
Z_LAG, X_LAG, P_LAG = 1, 2, 3


def iota(shape, axis):
    return lax.broadcasted_iota(jnp.int32, shape, axis)


def stick(rows, blocks, seqs_heads):
    carry = jnp.zeros((1, LANES), F32)
    carries = [carry]
    for row in rows[:0:-1]:
        carry = carry + row[:, blocks * LANES :]
        carries.append(carry)
    total = carry + rows[0][:, blocks * LANES :]
    factors = jnp.exp(jnp.concatenate(carries[::-1], axis=0))
    stacked = jnp.concatenate([row[:, : blocks * LANES] for row in rows], axis=0)
    parts = []
    for block in range(blocks):
        mine = stacked[:, block * LANES : (block + 1) * LANES] * factors[:, block : block + 1]
        parts.append(jnp.sum(mine, axis=0, keepdims=True))
    return jnp.concatenate(parts, axis=1), total


def kernel(
    shape,
    tokens,
    gain,
    key_weight,
    value_weight,
    bias,
    query,
    cache_out,
    bias_out,
    att_out,
    tok_v,
    weight_v,
    recv,
    normed,
    bias_v,
    bias_recv,
    query_v,
    query_f,
    gain_v,
    gain_f,
    perm,
    later_mask,
    parts,
    result,
    ready,
    load_sem,
    own_sem,
    bias_own_sem,
    z_send,
    z_recv,
    b_send,
    b_recv,
    x_send,
    x_recv,
    p_send,
    p_recv,
    part_send,
    part_recv,
    result_send,
    result_recv,
):
    n, cores, n_x, piece, seqs, heads, width, columns = shape
    steps = n // 2
    span = n // seqs
    rows = span * piece
    feat = width // (cores * n_x)
    head_size = columns // heads
    blocks = seqs * heads
    per_tile = LANES // piece
    z = lax.axis_index("sp")
    tp = lax.axis_index("tp")
    core = lax.rem(tp, cores)
    x = lax.div(tp, cores)
    partner = x * cores + (1 - core)
    mine = pl.ds(pl.multiple_of(tp * feat, feat), feat)

    rank = lax.rem(z + n - 1, n)

    def at_rank(r):
        return lax.rem(r + 1, n)

    barrier = pltpu.get_barrier_semaphore()

    def greet(higher, carry):
        pl.semaphore_signal(barrier, 1, device_id={"sp": at_rank(higher)}, device_id_type=MESH)
        return carry

    lax.fori_loop(rank + 1, n, greet, 0)
    for offset in range(1, n_x):
        pl.semaphore_signal(
            barrier, 1, device_id={"tp": lax.rem(x + offset, n_x) * cores + core}, device_id_type=MESH
        )
    pl.semaphore_signal(barrier, 1, device_id={"tp": partner}, device_id_type=MESH)

    loads = [
        pltpu.make_async_copy(gain, gain_v, load_sem.at[0]),
        pltpu.make_async_copy(bias, bias_v, load_sem.at[1]),
        pltpu.make_async_copy(query, query_v, load_sem.at[2]),
        pltpu.make_async_copy(tokens, tok_v, load_sem.at[3]),
        pltpu.make_async_copy(key_weight, weight_v.at[:, pl.ds(0, columns)], load_sem.at[4]),
        pltpu.make_async_copy(value_weight, weight_v.at[:, pl.ds(columns, columns)], load_sem.at[5]),
    ]
    for load in loads:
        load.start()
    own = pltpu.make_async_copy(tokens.at[z, :, mine], recv.at[0, core, x, pl.ds(0, piece)], own_sem)
    own.start()

    pl.semaphore_wait(barrier, rank + n_x)

    def z_copy(q):
        lower = q <= rank
        peer = jnp.where(lower, rank - q, q)
        slot = jnp.where(lower, rank, q - rank)
        to = at_rank(peer)
        return pltpu.make_async_remote_copy(
            tok_v.at[to, :, mine],
            recv.at[lax.div(slot, 2), core, x, pl.ds(pl.multiple_of(lax.rem(slot, 2) * piece, piece), piece)],
            z_send.at[q],
            z_recv.at[slot],
            device_id={"sp": to},
            device_id_type=MESH,
        )

    def z_arrival(q):
        return pltpu.make_async_remote_copy(
            tok_v.at[z, :, mine],
            recv.at[lax.div(q, 2), core, x, pl.ds(pl.multiple_of(lax.rem(q, 2) * piece, piece), piece)],
            z_send.at[q],
            z_recv.at[q],
            device_id={"sp": z},
            device_id_type=MESH,
        )

    def bias_copy(q):
        to = at_rank(jnp.where(q <= rank, rank - q, q))
        tile = lax.div(lax.rem(to, span), per_tile)
        return pltpu.make_async_remote_copy(
            bias_v.at[lax.div(to, span), :, pl.ds(pl.multiple_of(tile * LANES, LANES), LANES)],
            bias_recv.at[z],
            b_send,
            b_recv,
            device_id={"sp": to},
            device_id_type=MESH,
        )

    def x_copy(slot, offset):
        to = lax.rem(x + offset, n_x) * cores + core
        return pltpu.make_async_remote_copy(
            recv.at[slot, core, x],
            recv.at[slot, core, x],
            x_send.at[slot, offset - 1],
            x_recv.at[slot, offset - 1],
            device_id={"tp": to},
            device_id_type=MESH,
        )

    def x_arrival(slot, offset):
        came = lax.rem(x + n_x - offset, n_x)
        return pltpu.make_async_remote_copy(
            recv.at[slot, core, came],
            recv.at[slot, core, came],
            x_send.at[slot, offset - 1],
            x_recv.at[slot, offset - 1],
            device_id={"tp": partner},
            device_id_type=MESH,
        )

    def p_copy(slot):
        return pltpu.make_async_remote_copy(
            recv.at[slot, core], recv.at[slot, core], p_send.at[slot], p_recv.at[slot],
            device_id={"tp": partner}, device_id_type=MESH,
        )

    def p_arrival(slot):
        return pltpu.make_async_remote_copy(
            recv.at[slot, 1 - core], recv.at[slot, 1 - core], p_send.at[slot], p_recv.at[slot],
            device_id={"tp": partner}, device_id_type=MESH,
        )

    def part_copy():
        return pltpu.make_async_remote_copy(
            parts.at[rank], parts.at[rank], part_send, part_recv,
            device_id={"sp": at_rank(0)}, device_id_type=MESH,
        )

    def result_copy(r):
        return pltpu.make_async_remote_copy(
            result, result, result_send.at[r], result_recv, device_id={"sp": at_rank(r)}, device_id_type=MESH
        )

    for load in loads:
        load.wait()

    def send(q):
        z_copy(q).start()
        bias_copy(q).start()

    def answer(q, carry):
        pl.semaphore_signal(ready.at[rank], 1, device_id={"sp": at_rank(rank - q)}, device_id_type=MESH)
        send(q)
        return carry

    lax.fori_loop(1, rank + 1, answer, 0)
    out_row, in_row = iota((4 * 2 * piece, 4 * 2 * piece), 0), iota((4 * 2 * piece, 4 * 2 * piece), 1)
    source = (
        lax.rem(out_row, 2) * (4 * piece)
        + lax.rem(lax.div(out_row, 2), 2) * (2 * piece)
        + lax.div(out_row, 4)
    )
    perm[...] = jnp.where(in_row == source, 1.0, 0.0).astype(BF16)
    later_mask[...] = jnp.where(iota((rows, rows), 0) > iota((rows, rows), 1), 1.0, 0.0).astype(BF16)

    gains = gain_v[...].astype(F32)
    for t in range(cores * n_x):
        gain_f[t] = jnp.concatenate(
            [gains[t * feat // LANES + j : t * feat // LANES + j + 1] for j in range(feat // LANES)], axis=1
        )
    queries = query_v[...].astype(F32)
    for s in range(seqs):
        query_f[s] = queries[s : s + 1]

    def project(piece_of, count):
        squares = jnp.zeros((count, feat), F32)
        for t in range(cores * n_x):
            value = piece_of(t).astype(F32)
            squares = squares + value * value
        inverse = lax.rsqrt(jnp.sum(squares, axis=1, keepdims=True) / width + norm_eps)
        for t in range(cores * n_x):
            value = piece_of(t).astype(F32) * inverse * gain_f[t]
            normed[pl.ds(0, count), pl.ds(t * feat, feat)] = value.astype(BF16)
        return jnp.dot(normed[pl.ds(0, count), :], weight_v[...], preferred_element_type=F32).astype(BF16)

    lane = iota((1, LANES), 1)

    def own_read(s, totals):
        projected = project(
            lambda t: tok_v[pl.ds(s * span, span), :, pl.ds(t * feat, feat)].reshape(rows, feat), rows
        )
        keys, values = projected[:, :columns], projected[:, columns:]
        head_row, head_lane = iota((8, columns), 0), lax.div(iota((8, columns), 1), head_size)
        spread = jnp.where(head_row == head_lane, query_f[s], 0.0).astype(BF16)
        logits = lax.dot_general(spread, keys, (((1,), (1,)), ((), ())), preferred_element_type=F32)
        terms = jnp.concatenate([bias_v[s].astype(F32), jnp.zeros((8 - heads, rows), F32)], axis=0)
        logits = logits * head_size ** (-0.5) + terms
        soft = jnp.log1p(jnp.exp(-jnp.abs(logits)))
        keep = jnp.minimum(-logits, 0.0) - soft
        take = jnp.minimum(logits, 0.0) - soft
        high = keep.astype(BF16).astype(F32)
        middle = (keep - high).astype(BF16).astype(F32)
        low = keep - high - middle
        split = jnp.concatenate([high, middle, low, jnp.zeros_like(low)], axis=0).astype(BF16)
        sums = jnp.dot(split, later_mask[...], preferred_element_type=F32)
        later = sums[0:8] + sums[8:16] + sums[16:24]
        weights = jnp.exp(take + later)
        high = weights.astype(BF16).astype(F32)
        split = jnp.concatenate([high, weights - high], axis=0).astype(BF16)
        mixed = jnp.dot(split, values, preferred_element_type=F32)
        mixed = mixed[0:8] + mixed[8:16]
        read = jnp.sum(jnp.where(head_row == head_lane, mixed, 0.0), axis=0, keepdims=True)
        parts[rank, :, pl.ds(pl.multiple_of(s * columns, columns), columns)] = read
        total = jnp.sum(keep, axis=1, keepdims=True)
        for h in range(heads):
            totals = totals + jnp.where(lane == s * heads + h, total[h : h + 1], 0.0)
        return totals

    own_tile = lax.div(lax.rem(z, span), per_tile)
    own_bias = pltpu.make_async_copy(
        bias.at[lax.div(z, span), :, pl.ds(pl.multiple_of(own_tile * LANES, LANES), LANES)],
        bias_recv.at[z],
        bias_own_sem,
    )
    own_bias.start()
    own.wait()

    def higher(q):
        @pl.when((q > rank) & (q < n))
        def _():
            pl.semaphore_wait(ready.at[q], 1)
            send(q)

    def step(k, totals):
        higher(rank + 1 + 2 * k)
        higher(rank + 2 + 2 * k)

        totals = lax.cond(k < seqs, own_read, lambda s, t: t, k, totals)

        @pl.when(k == seqs - 1)
        def _():
            parts[rank, :, pl.ds(blocks * LANES, LANES)] = totals

            @pl.when(rank > 0)
            def _():
                part_copy().start()

        @pl.when((k >= Z_LAG) & (k < steps + Z_LAG))
        def _():
            slot = k - Z_LAG

            @pl.when(slot > 0)
            def _():
                z_arrival(2 * slot).wait_recv()

            z_arrival(2 * slot + 1).wait_recv()
            for offset in range(1, n_x):
                x_copy(slot, offset).start()

        @pl.when((k >= X_LAG) & (k < steps + X_LAG))
        def _():
            for offset in range(1, n_x):
                x_arrival(k - X_LAG, offset).wait_recv()
            p_copy(k - X_LAG).start()

        @pl.when(k >= P_LAG)
        def _():
            slot = k - P_LAG
            p_arrival(slot).wait_recv()
            projected = project(lambda t: recv[slot, t % cores, t // cores], 2 * piece)
            stacked = jnp.concatenate(
                [projected[:, j * LANES : (j + 1) * LANES] for j in range(2 * columns // LANES)], axis=0
            )
            placed = jnp.dot(perm[...], stacked, preferred_element_type=F32).astype(BF16)
            for half in range(2):
                q = 2 * slot + half
                at = at_rank(jnp.where(q <= rank, rank - q, q))
                cache_out[pl.ds(pl.multiple_of(at * 4 * piece, 4 * piece), 4 * piece)] = placed[
                    half * 4 * piece : (half + 1) * 4 * piece
                ]

        return totals

    lax.fori_loop(0, steps + P_LAG, step, jnp.zeros((1, LANES), F32))

    @pl.when(rank == 0)
    def _():
        others = parts.at[pl.ds(1, n - 1)]
        pltpu.make_async_copy(others, others, part_recv).wait()
        by_position = [parts[(j + n - 1) % n] for j in range(n)]
        result[...] = stick(by_position, blocks, seqs)[0]

        def tell(r, carry):
            result_copy(r).start()
            return carry

        lax.fori_loop(1, n, tell, 0)

    own_bias.wait()
    others = pl.ds(0, n - 1)
    pltpu.make_async_copy(bias_recv.at[others], bias_recv.at[others], b_recv).wait()
    arrived = bias_recv[...].astype(F32)
    part = lax.rem(lax.rem(z, span), per_tile)
    chosen = arrived[:, :, 0:piece]
    for j in range(1, per_tile):
        chosen = jnp.where(part == j, arrived[:, :, j * piece : (j + 1) * piece], chosen)
    bias_out[...] = chosen.astype(BF16)

    @pl.when(rank > 0)
    def _():
        result_copy(0).wait_recv()

    for s in range(seqs):
        att_out[pl.ds(s, 1), :] = result[:, s * columns : (s + 1) * columns]

    pltpu.make_async_copy(bias_recv.at[others], bias_recv.at[others], b_send).wait()

    @pl.when(rank > 0)
    def _():
        part_copy().wait_send()

    @pl.when(rank == 0)
    def _():
        def told(r, carry):
            result_copy(r).wait_send()
            return carry

        lax.fori_loop(1, n, told, 0)

    def drain(slot, carry):
        for offset in range(1, n_x):
            x_copy(slot, offset).wait_send()
        p_copy(slot).wait_send()

        @pl.when(slot > 0)
        def _():
            z_copy(2 * slot).wait_send()

        z_copy(2 * slot + 1).wait_send()
        return carry

    lax.fori_loop(0, steps, drain, 0)


def local(cores, tokens, norm_gain, key_weight, value_weight, break_bias, new_query):
    seqs, tok_rows, width = tokens.shape
    heads = break_bias.shape[2]
    columns = key_weight.shape[1]
    n = lax.axis_size("sp")
    n_tp = lax.axis_size("tp")
    n_x = n_tp // cores
    piece = tok_rows * seqs // n
    span = n // seqs
    steps = n // 2
    feat = width // n_tp
    shape = (n, cores, n_x, piece, seqs, heads, width, columns)
    dma = pltpu.SemaphoreType.DMA
    message = seqs * columns + LANES
    cache, bias_out, attended = pl.pallas_call(
        functools.partial(kernel, shape),
        out_shape=(
            jax.ShapeDtypeStruct((n * piece * 4, LANES), BF16),
            jax.ShapeDtypeStruct((n, heads, piece), BF16),
            jax.ShapeDtypeStruct((seqs, columns), F32),
        ),
        in_specs=[pl.BlockSpec(memory_space=pltpu.HBM)] * 6,
        out_specs=[pl.BlockSpec(memory_space=pltpu.VMEM)] * 3,
        scratch_shapes=[
            pltpu.VMEM((n, piece, width), BF16),
            pltpu.VMEM((width, 2 * columns), BF16),
            pltpu.VMEM((steps, cores, n_x, 2 * piece, feat), BF16),
            pltpu.VMEM((max(span, 2) * piece, width), BF16),
            pltpu.VMEM((seqs, heads, tok_rows), BF16),
            pltpu.VMEM((n, heads, LANES), BF16),
            pltpu.VMEM((seqs, columns), BF16),
            pltpu.VMEM((seqs, 1, columns), F32),
            pltpu.VMEM((width // LANES, LANES), BF16),
            pltpu.VMEM((n_tp, 1, feat), F32),
            pltpu.VMEM((8 * piece, 8 * piece), BF16),
            pltpu.VMEM((tok_rows, tok_rows), BF16),
            pltpu.VMEM((n, 1, message), F32),
            pltpu.VMEM((1, seqs * columns), F32),
            pltpu.SemaphoreType.REGULAR((n,)),
            dma((6,)),
            dma,
            dma,
            dma((n,)),
            dma((n,)),
            dma,
            dma,
            dma((steps, n_x - 1)),
            dma((steps, n_x - 1)),
            dma((steps,)),
            dma((steps,)),
            dma,
            dma,
            dma((n,)),
            dma,
        ],
        compiler_params=pltpu.CompilerParams(
            collective_id=0, has_side_effects=True, vmem_limit_bytes=61000000
        ),
    )(
        tokens.reshape(n, piece, width),
        norm_gain.reshape(width // LANES, LANES),
        key_weight,
        value_weight,
        jnp.transpose(break_bias, (0, 2, 1)),
        new_query,
    )
    halves = columns // LANES
    paired = cache.reshape(n, piece, halves, 2, LANES)
    paired = jnp.transpose(paired, (0, 1, 3, 2, 4)).reshape(n, piece, 2, columns)
    return (paired[None], jnp.transpose(bias_out, (0, 2, 1))[None], attended)


def solution(mesh):
    return jax.shard_map(
        functools.partial(local, 2),
        mesh=mesh,
        in_specs=(
            P("grp", "sp", None),
            P(),
            P(None, "tp"),
            P(None, "tp"),
            P("grp", "sp", "tp"),
            P("grp", "tp"),
        ),
        out_specs=(
            P(("grp", "sp"), None, None, None, "tp"),
            P(("grp", "sp"), None, None, "tp"),
            P("grp", "tp"),
        ),
        check_vma=False,
    )
```

```python
import functools

import jax
import jax.numpy as jnp
from jax import lax
from jax.experimental import pallas as pl
from jax.experimental.pallas import tpu as pltpu
from jax.sharding import PartitionSpec as P

norm_eps = 1e-06
LANES = 128
MESH = pl.DeviceIdType.MESH
F32 = jnp.float32
BF16 = jnp.bfloat16
Z_LAG, X_LAG, FAR_LAG, P_LAG = 4, 7, 10, 13
FIRST = 10


def iota(shape, axis):
    return lax.broadcasted_iota(jnp.int32, shape, axis)


def stick(rows, blocks, seqs_heads):
    carry = jnp.zeros((1, LANES), F32)
    carries = [carry]
    for row in rows[:0:-1]:
        carry = carry + row[:, blocks * LANES :]
        carries.append(carry)
    total = carry + rows[0][:, blocks * LANES :]
    factors = jnp.exp(jnp.concatenate(carries[::-1], axis=0))
    stacked = jnp.concatenate([row[:, : blocks * LANES] for row in rows], axis=0)
    parts = []
    for block in range(blocks):
        mine = stacked[:, block * LANES : (block + 1) * LANES] * factors[:, block : block + 1]
        parts.append(jnp.sum(mine, axis=0, keepdims=True))
    return jnp.concatenate(parts, axis=1), total


def kernel(
    shape,
    tokens,
    gain,
    key_weight,
    value_weight,
    bias,
    query,
    cache_out,
    bias_out,
    att_out,
    tok_v,
    weight_v,
    recv,
    normed,
    bias_v,
    bias_recv,
    query_v,
    query_f,
    gain_v,
    gain_f,
    perm,
    later_mask,
    parts,
    result,
    ready,
    load_sem,
    own_sem,
    bias_own_sem,
    z_send,
    z_recv,
    b_send,
    b_recv,
    x_send,
    x_recv,
    far_send,
    far_recv,
    p_send,
    p_recv,
    part_send,
    part_recv,
    result_send,
    result_recv,
):
    n, cores, n_x, piece, seqs, heads, width, columns = shape
    steps = n // 2
    span = n // seqs
    rows = span * piece
    feat = width // (cores * n_x)
    head_size = columns // heads
    blocks = seqs * heads
    per_tile = LANES // piece
    z = lax.axis_index("sp")
    tp = lax.axis_index("tp")
    core = lax.rem(tp, cores)
    x = lax.div(tp, cores)
    partner = x * cores + (1 - core)
    mine = pl.ds(pl.multiple_of(tp * feat, feat), feat)

    late = n * 3 // 8
    rank = jnp.where(z == 0, late, jnp.where(z <= late, z - 1, z))

    def at_rank(r):
        return jnp.where(r == late, 0, jnp.where(r < late, r + 1, r))

    barrier = pltpu.get_barrier_semaphore()

    def greet(higher, carry):
        pl.semaphore_signal(barrier, 1, device_id={"sp": at_rank(higher)}, device_id_type=MESH)
        return carry

    lax.fori_loop(rank + 1, n, greet, 0)
    for offset in range(1, n_x):
        pl.semaphore_signal(
            barrier, 1, device_id={"tp": lax.rem(x + offset, n_x) * cores + core}, device_id_type=MESH
        )
    pl.semaphore_signal(barrier, 1, device_id={"tp": partner}, device_id_type=MESH)

    loads = [
        pltpu.make_async_copy(gain, gain_v, load_sem.at[0]),
        pltpu.make_async_copy(bias, bias_v, load_sem.at[1]),
        pltpu.make_async_copy(query, query_v, load_sem.at[2]),
        pltpu.make_async_copy(tokens, tok_v, load_sem.at[3]),
        pltpu.make_async_copy(key_weight, weight_v.at[:, pl.ds(0, columns)], load_sem.at[4]),
        pltpu.make_async_copy(value_weight, weight_v.at[:, pl.ds(columns, columns)], load_sem.at[5]),
    ]
    for load in loads:
        load.start()
    own = pltpu.make_async_copy(tokens.at[z, :, mine], recv.at[0, core, x, pl.ds(0, piece)], own_sem)
    own.start()

    pl.semaphore_wait(barrier, rank + n_x)

    def report(q, carry):
        pl.semaphore_signal(ready.at[rank], 1, device_id={"sp": at_rank(rank - q)}, device_id_type=MESH)
        return carry

    lax.fori_loop(1, rank + 1, report, 0)

    def z_copy(q):
        lower = q <= rank
        peer = jnp.where(lower, rank - q, q)
        slot = jnp.where(lower, rank, q - rank)
        to = at_rank(peer)
        return pltpu.make_async_remote_copy(
            tok_v.at[to, :, mine],
            recv.at[lax.div(slot, 2), core, x, pl.ds(pl.multiple_of(lax.rem(slot, 2) * piece, piece), piece)],
            z_send.at[q],
            z_recv.at[slot],
            device_id={"sp": to},
            device_id_type=MESH,
        )

    def z_arrival(q):
        return pltpu.make_async_remote_copy(
            tok_v.at[z, :, mine],
            recv.at[lax.div(q, 2), core, x, pl.ds(pl.multiple_of(lax.rem(q, 2) * piece, piece), piece)],
            z_send.at[q],
            z_recv.at[q],
            device_id={"sp": z},
            device_id_type=MESH,
        )

    def bias_copy(q):
        to = at_rank(jnp.where(q <= rank, rank - q, q))
        tile = lax.div(lax.rem(to, span), per_tile)
        return pltpu.make_async_remote_copy(
            bias_v.at[lax.div(to, span), :, pl.ds(pl.multiple_of(tile * LANES, LANES), LANES)],
            bias_recv.at[z],
            b_send,
            b_recv,
            device_id={"sp": to},
            device_id_type=MESH,
        )

    def x_copy(slot, way):
        to = lax.rem(x + (1 if way == 0 else n_x - 1), n_x) * cores + core
        return pltpu.make_async_remote_copy(
            recv.at[slot, core, x],
            recv.at[slot, core, x],
            x_send.at[slot, way],
            x_recv.at[slot, way],
            device_id={"tp": to},
            device_id_type=MESH,
        )

    def x_arrival(slot, way):
        came = lax.rem(x + (n_x - 1 if way == 0 else 1), n_x)
        return pltpu.make_async_remote_copy(
            recv.at[slot, core, came],
            recv.at[slot, core, came],
            x_send.at[slot, way],
            x_recv.at[slot, way],
            device_id={"tp": partner},
            device_id_type=MESH,
        )

    def far_ref(slot, way, chip):
        return recv.at[slot, core, chip, pl.ds(way * piece, piece)]

    def far_copy(slot, way):
        came = lax.rem(x + (n_x - 1 if way == 0 else 1), n_x)
        to = lax.rem(x + (1 if way == 0 else n_x - 1), n_x) * cores + core
        return pltpu.make_async_remote_copy(
            far_ref(slot, way, came),
            far_ref(slot, way, came),
            far_send.at[slot, way],
            far_recv.at[slot, way],
            device_id={"tp": to},
            device_id_type=MESH,
        )

    def far_arrival(slot, way):
        came = lax.rem(x + 2, n_x)
        return pltpu.make_async_remote_copy(
            far_ref(slot, way, came),
            far_ref(slot, way, came),
            far_send.at[slot, way],
            far_recv.at[slot, way],
            device_id={"tp": partner},
            device_id_type=MESH,
        )

    def p_copy(slot):
        return pltpu.make_async_remote_copy(
            recv.at[slot, core], recv.at[slot, core], p_send.at[slot], p_recv.at[slot],
            device_id={"tp": partner}, device_id_type=MESH,
        )

    def p_arrival(slot):
        return pltpu.make_async_remote_copy(
            recv.at[slot, 1 - core], recv.at[slot, 1 - core], p_send.at[slot], p_recv.at[slot],
            device_id={"tp": partner}, device_id_type=MESH,
        )

    def part_copy():
        return pltpu.make_async_remote_copy(
            parts.at[rank], parts.at[rank], part_send, part_recv,
            device_id={"sp": at_rank(0)}, device_id_type=MESH,
        )

    def result_copy(r):
        return pltpu.make_async_remote_copy(
            result, result, result_send.at[r], result_recv, device_id={"sp": at_rank(r)}, device_id_type=MESH
        )

    for load in loads:
        load.wait()

    def send(q):
        z_copy(q).start()
        bias_copy(q).start()

    def answer(r, carry):
        first = jnp.where(r == 0, late, jnp.where(r <= late, r - 1, r))
        send(rank - jnp.where(rank > late, first, r))
        return carry

    lax.fori_loop(0, jnp.minimum(rank, FIRST), answer, 0)
    out_row, in_row = iota((4 * 2 * piece, 4 * 2 * piece), 0), iota((4 * 2 * piece, 4 * 2 * piece), 1)
    source = (
        lax.rem(out_row, 2) * (4 * piece)
        + lax.rem(lax.div(out_row, 2), 2) * (2 * piece)
        + lax.div(out_row, 4)
    )
    perm[...] = jnp.where(in_row == source, 1.0, 0.0).astype(BF16)
    later_mask[...] = jnp.where(iota((rows, rows), 0) > iota((rows, rows), 1), 1.0, 0.0).astype(BF16)

    gains = gain_v[...].astype(F32)
    for t in range(cores * n_x):
        gain_f[t] = jnp.concatenate(
            [gains[t * feat // LANES + j : t * feat // LANES + j + 1] for j in range(feat // LANES)], axis=1
        )
    queries = query_v[...].astype(F32)
    for s in range(seqs):
        query_f[s] = queries[s : s + 1]

    def project(piece_of, count):
        squares = jnp.zeros((count, feat), F32)
        for t in range(cores * n_x):
            value = piece_of(t).astype(F32)
            squares = squares + value * value
        inverse = lax.rsqrt(jnp.sum(squares, axis=1, keepdims=True) / width + norm_eps)
        for t in range(cores * n_x):
            value = piece_of(t).astype(F32) * inverse * gain_f[t]
            normed[pl.ds(0, count), pl.ds(t * feat, feat)] = value.astype(BF16)
        return jnp.dot(normed[pl.ds(0, count), :], weight_v[...], preferred_element_type=F32).astype(BF16)

    lane = iota((1, LANES), 1)

    def own_read(s, totals):
        projected = project(
            lambda t: tok_v[pl.ds(s * span, span), :, pl.ds(t * feat, feat)].reshape(rows, feat), rows
        )
        keys, values = projected[:, :columns], projected[:, columns:]
        head_row, head_lane = iota((8, columns), 0), lax.div(iota((8, columns), 1), head_size)
        spread = jnp.where(head_row == head_lane, query_f[s], 0.0).astype(BF16)
        logits = lax.dot_general(spread, keys, (((1,), (1,)), ((), ())), preferred_element_type=F32)
        terms = jnp.concatenate([bias_v[s].astype(F32), jnp.zeros((8 - heads, rows), F32)], axis=0)
        logits = logits * head_size ** (-0.5) + terms
        soft = jnp.log1p(jnp.exp(-jnp.abs(logits)))
        keep = jnp.minimum(-logits, 0.0) - soft
        take = jnp.minimum(logits, 0.0) - soft
        high = keep.astype(BF16).astype(F32)
        middle = (keep - high).astype(BF16).astype(F32)
        low = keep - high - middle
        split = jnp.concatenate([high, middle, low, jnp.zeros_like(low)], axis=0).astype(BF16)
        sums = jnp.dot(split, later_mask[...], preferred_element_type=F32)
        later = sums[0:8] + sums[8:16] + sums[16:24]
        weights = jnp.exp(take + later)
        high = weights.astype(BF16).astype(F32)
        split = jnp.concatenate([high, weights - high], axis=0).astype(BF16)
        mixed = jnp.dot(split, values, preferred_element_type=F32)
        mixed = mixed[0:8] + mixed[8:16]
        read = jnp.sum(jnp.where(head_row == head_lane, mixed, 0.0), axis=0, keepdims=True)
        parts[rank, :, pl.ds(pl.multiple_of(s * columns, columns), columns)] = read
        total = jnp.sum(keep, axis=1, keepdims=True)
        for h in range(heads):
            totals = totals + jnp.where(lane == s * heads + h, total[h : h + 1], 0.0)
        return totals

    own_tile = lax.div(lax.rem(z, span), per_tile)
    own_bias = pltpu.make_async_copy(
        bias.at[lax.div(z, span), :, pl.ds(pl.multiple_of(own_tile * LANES, LANES), LANES)],
        bias_recv.at[z],
        bias_own_sem,
    )
    own_bias.start()
    own.wait()

    parts[rank, :, pl.ds(blocks * LANES, LANES)] = lax.fori_loop(0, seqs, own_read, jnp.zeros((1, LANES), F32))

    @pl.when(rank > 0)
    def _():
        part_copy().start()

    lax.fori_loop(jnp.minimum(rank, FIRST), rank, answer, 0)

    def higher(q):
        @pl.when((q > rank) & (q < n))
        def _():
            pl.semaphore_wait(ready.at[q], 1)
            send(q)

    def step(k, carry):
        higher(rank + 1 + 2 * k)
        higher(rank + 2 + 2 * k)

        @pl.when(k >= P_LAG)
        def _():
            slot = k - P_LAG
            p_arrival(slot).wait_recv()
            projected = project(lambda t: recv[slot, t % cores, t // cores], 2 * piece)
            stacked = jnp.concatenate(
                [projected[:, j * LANES : (j + 1) * LANES] for j in range(2 * columns // LANES)], axis=0
            )
            placed = jnp.dot(perm[...], stacked, preferred_element_type=F32).astype(BF16)
            for half in range(2):
                q = 2 * slot + half
                at = at_rank(jnp.where(q <= rank, rank - q, q))
                cache_out[pl.ds(pl.multiple_of(at * 4 * piece, 4 * piece), 4 * piece)] = placed[
                    half * 4 * piece : (half + 1) * 4 * piece
                ]

        @pl.when((k >= FAR_LAG) & (k < steps + FAR_LAG))
        def _():
            slot = k - FAR_LAG
            for way in range(2):
                far_arrival(slot, way).wait_recv()
            p_copy(slot).start()

        @pl.when((k >= X_LAG) & (k < steps + X_LAG))
        def _():
            slot = k - X_LAG
            for way in range(2):
                x_arrival(slot, way).wait_recv()
                far_copy(slot, way).start()

        @pl.when((k >= Z_LAG) & (k < steps + Z_LAG))
        def _():
            slot = k - Z_LAG

            @pl.when(slot > 0)
            def _():
                z_arrival(2 * slot).wait_recv()

            z_arrival(2 * slot + 1).wait_recv()
            for way in range(2):
                x_copy(slot, way).start()

        return carry

    lax.fori_loop(0, steps + P_LAG, step, 0)

    @pl.when(rank == 0)
    def _():
        others = parts.at[pl.ds(1, n - 1)]
        pltpu.make_async_copy(others, others, part_recv).wait()
        by_position = [parts[late if j == 0 else j - 1 if j <= late else j] for j in range(n)]
        result[...] = stick(by_position, blocks, seqs)[0]

        def tell(r, carry):
            result_copy(r).start()
            return carry

        lax.fori_loop(1, n, tell, 0)

    own_bias.wait()
    others = pl.ds(0, n - 1)
    pltpu.make_async_copy(bias_recv.at[others], bias_recv.at[others], b_recv).wait()
    arrived = bias_recv[...].astype(F32)
    part = lax.rem(lax.rem(z, span), per_tile)
    chosen = arrived[:, :, 0:piece]
    for j in range(1, per_tile):
        chosen = jnp.where(part == j, arrived[:, :, j * piece : (j + 1) * piece], chosen)
    bias_out[...] = chosen.astype(BF16)

    @pl.when(rank > 0)
    def _():
        result_copy(0).wait_recv()

    for s in range(seqs):
        att_out[pl.ds(s, 1), :] = result[:, s * columns : (s + 1) * columns]

    pltpu.make_async_copy(bias_recv.at[others], bias_recv.at[others], b_send).wait()

    @pl.when(rank > 0)
    def _():
        part_copy().wait_send()

    @pl.when(rank == 0)
    def _():
        def told(r, carry):
            result_copy(r).wait_send()
            return carry

        lax.fori_loop(1, n, told, 0)

    def drain(slot, carry):
        for way in range(2):
            x_copy(slot, way).wait_send()
            far_copy(slot, way).wait_send()
        p_copy(slot).wait_send()

        @pl.when(slot > 0)
        def _():
            z_copy(2 * slot).wait_send()

        z_copy(2 * slot + 1).wait_send()
        return carry

    lax.fori_loop(0, steps, drain, 0)


def local(cores, tokens, norm_gain, key_weight, value_weight, break_bias, new_query):
    seqs, tok_rows, width = tokens.shape
    heads = break_bias.shape[2]
    columns = key_weight.shape[1]
    n = lax.axis_size("sp")
    n_tp = lax.axis_size("tp")
    n_x = n_tp // cores
    piece = tok_rows * seqs // n
    span = n // seqs
    steps = n // 2
    feat = width // n_tp
    shape = (n, cores, n_x, piece, seqs, heads, width, columns)
    dma = pltpu.SemaphoreType.DMA
    message = seqs * columns + LANES
    cache, bias_out, attended = pl.pallas_call(
        functools.partial(kernel, shape),
        out_shape=(
            jax.ShapeDtypeStruct((n * piece * 4, LANES), BF16),
            jax.ShapeDtypeStruct((n, heads, piece), BF16),
            jax.ShapeDtypeStruct((seqs, columns), F32),
        ),
        in_specs=[pl.BlockSpec(memory_space=pltpu.HBM)] * 6,
        out_specs=[pl.BlockSpec(memory_space=pltpu.VMEM)] * 3,
        scratch_shapes=[
            pltpu.VMEM((n, piece, width), BF16),
            pltpu.VMEM((width, 2 * columns), BF16),
            pltpu.VMEM((steps, cores, n_x, 2 * piece, feat), BF16),
            pltpu.VMEM((max(span, 2) * piece, width), BF16),
            pltpu.VMEM((seqs, heads, tok_rows), BF16),
            pltpu.VMEM((n, heads, LANES), BF16),
            pltpu.VMEM((seqs, columns), BF16),
            pltpu.VMEM((seqs, 1, columns), F32),
            pltpu.VMEM((width // LANES, LANES), BF16),
            pltpu.VMEM((n_tp, 1, feat), F32),
            pltpu.VMEM((8 * piece, 8 * piece), BF16),
            pltpu.VMEM((tok_rows, tok_rows), BF16),
            pltpu.VMEM((n, 1, message), F32),
            pltpu.VMEM((1, seqs * columns), F32),
            pltpu.SemaphoreType.REGULAR((n,)),
            dma((6,)),
            dma,
            dma,
            dma((n,)),
            dma((n,)),
            dma,
            dma,
            dma((steps, 2)),
            dma((steps, 2)),
            dma((steps, 2)),
            dma((steps, 2)),
            dma((steps,)),
            dma((steps,)),
            dma,
            dma,
            dma((n,)),
            dma,
        ],
        compiler_params=pltpu.CompilerParams(
            collective_id=0, has_side_effects=True, vmem_limit_bytes=48 * 1024 * 1024
        ),
    )(
        *(
            pltpu.with_memory_space_constraint(array, pltpu.HBM)
            for array in (
                tokens.reshape(n, piece, width),
                norm_gain.reshape(width // LANES, LANES),
                key_weight,
                value_weight,
                jnp.transpose(break_bias, (0, 2, 1)),
                new_query,
            )
        )
    )
    halves = columns // LANES
    paired = cache.reshape(n, piece, halves, 2, LANES)
    paired = jnp.transpose(paired, (0, 1, 3, 2, 4)).reshape(n, piece, 2, columns)
    return (paired[None], jnp.transpose(bias_out, (0, 2, 1))[None], attended)


def solution(mesh):
    return jax.shard_map(
        functools.partial(local, 2),
        mesh=mesh,
        in_specs=(
            P("grp", "sp", None),
            P(),
            P(None, "tp"),
            P(None, "tp"),
            P("grp", "sp", "tp"),
            P("grp", "tp"),
        ),
        out_specs=(
            P(("grp", "sp"), None, None, None, "tp"),
            P(("grp", "sp"), None, None, "tp"),
            P("grp", "tp"),
        ),
        check_vma=False,
    )
```

```python
import functools

import jax
import jax.numpy as jnp
from jax import lax
from jax.experimental import pallas as pl
from jax.experimental.pallas import tpu as pltpu
from jax.sharding import PartitionSpec as P

norm_eps = 1e-06
LANES = 128
MESH = pl.DeviceIdType.MESH
F32 = jnp.float32
BF16 = jnp.bfloat16
Z_LAG, X_LAG, FAR_LAG, P_LAG = 4, 7, 10, 13
FIRST = 10


def iota(shape, axis):
    return lax.broadcasted_iota(jnp.int32, shape, axis)


def stick(rows, blocks, seqs_heads):
    carry = jnp.zeros((1, LANES), F32)
    carries = [carry]
    for row in rows[:0:-1]:
        carry = carry + row[:, blocks * LANES :]
        carries.append(carry)
    total = carry + rows[0][:, blocks * LANES :]
    factors = jnp.exp(jnp.concatenate(carries[::-1], axis=0))
    stacked = jnp.concatenate([row[:, : blocks * LANES] for row in rows], axis=0)
    parts = []
    for block in range(blocks):
        mine = stacked[:, block * LANES : (block + 1) * LANES] * factors[:, block : block + 1]
        parts.append(jnp.sum(mine, axis=0, keepdims=True))
    return jnp.concatenate(parts, axis=1), total


def kernel(
    shape,
    tokens,
    gain,
    key_weight,
    value_weight,
    bias,
    query,
    cache_out,
    bias_out,
    att_out,
    tok_v,
    weight_v,
    recv,
    normed,
    bias_v,
    bias_recv,
    query_v,
    query_f,
    gain_v,
    gain_f,
    perm,
    later_mask,
    parts,
    result,
    ready,
    load_sem,
    own_sem,
    bias_own_sem,
    z_send,
    z_recv,
    b_send,
    b_recv,
    x_send,
    x_recv,
    far_send,
    far_recv,
    p_send,
    p_recv,
    part_send,
    part_recv,
    result_send,
    result_recv,
):
    n, cores, n_x, piece, seqs, heads, width, columns = shape
    steps = n // 2
    span = n // seqs
    rows = span * piece
    feat = width // (cores * n_x)
    head_size = columns // heads
    blocks = seqs * heads
    per_tile = LANES // piece
    z = lax.axis_index("sp")
    tp = lax.axis_index("tp")
    core = lax.rem(tp, cores)
    x = lax.div(tp, cores)
    partner = x * cores + (1 - core)
    mine = pl.ds(pl.multiple_of(tp * feat, feat), feat)

    late = n // 4
    rank = jnp.where(z == 0, late, jnp.where(z <= late, z - 1, z))

    def at_rank(r):
        return jnp.where(r == late, 0, jnp.where(r < late, r + 1, r))

    barrier = pltpu.get_barrier_semaphore()

    def greet(higher, carry):
        pl.semaphore_signal(barrier, 1, device_id={"sp": at_rank(higher)}, device_id_type=MESH)
        return carry

    lax.fori_loop(rank + 1, n, greet, 0)
    for offset in range(1, n_x):
        pl.semaphore_signal(
            barrier, 1, device_id={"tp": lax.rem(x + offset, n_x) * cores + core}, device_id_type=MESH
        )
    pl.semaphore_signal(barrier, 1, device_id={"tp": partner}, device_id_type=MESH)

    loads = [
        pltpu.make_async_copy(gain, gain_v, load_sem.at[0]),
        pltpu.make_async_copy(bias, bias_v, load_sem.at[1]),
        pltpu.make_async_copy(query, query_v, load_sem.at[2]),
        pltpu.make_async_copy(tokens, tok_v, load_sem.at[3]),
        pltpu.make_async_copy(key_weight, weight_v.at[:, pl.ds(0, columns)], load_sem.at[4]),
        pltpu.make_async_copy(value_weight, weight_v.at[:, pl.ds(columns, columns)], load_sem.at[5]),
    ]
    for load in loads:
        load.start()
    own = pltpu.make_async_copy(tokens.at[z, :, mine], recv.at[0, core, x, pl.ds(0, piece)], own_sem)
    own.start()

    pl.semaphore_wait(barrier, rank + n_x)

    def report(q, carry):
        pl.semaphore_signal(ready.at[rank], 1, device_id={"sp": at_rank(rank - q)}, device_id_type=MESH)
        return carry

    lax.fori_loop(1, rank + 1, report, 0)

    def z_copy(q):
        lower = q <= rank
        peer = jnp.where(lower, rank - q, q)
        slot = jnp.where(lower, rank, q - rank)
        to = at_rank(peer)
        return pltpu.make_async_remote_copy(
            tok_v.at[to, :, mine],
            recv.at[lax.div(slot, 2), core, x, pl.ds(pl.multiple_of(lax.rem(slot, 2) * piece, piece), piece)],
            z_send.at[q],
            z_recv.at[slot],
            device_id={"sp": to},
            device_id_type=MESH,
        )

    def z_arrival(q):
        return pltpu.make_async_remote_copy(
            tok_v.at[z, :, mine],
            recv.at[lax.div(q, 2), core, x, pl.ds(pl.multiple_of(lax.rem(q, 2) * piece, piece), piece)],
            z_send.at[q],
            z_recv.at[q],
            device_id={"sp": z},
            device_id_type=MESH,
        )

    def bias_copy(q):
        to = at_rank(jnp.where(q <= rank, rank - q, q))
        tile = lax.div(lax.rem(to, span), per_tile)
        return pltpu.make_async_remote_copy(
            bias_v.at[lax.div(to, span), :, pl.ds(pl.multiple_of(tile * LANES, LANES), LANES)],
            bias_recv.at[z],
            b_send,
            b_recv,
            device_id={"sp": to},
            device_id_type=MESH,
        )

    def x_copy(slot, way):
        to = lax.rem(x + (1 if way == 0 else n_x - 1), n_x) * cores + core
        return pltpu.make_async_remote_copy(
            recv.at[slot, core, x],
            recv.at[slot, core, x],
            x_send.at[slot, way],
            x_recv.at[slot, way],
            device_id={"tp": to},
            device_id_type=MESH,
        )

    def x_arrival(slot, way):
        came = lax.rem(x + (n_x - 1 if way == 0 else 1), n_x)
        return pltpu.make_async_remote_copy(
            recv.at[slot, core, came],
            recv.at[slot, core, came],
            x_send.at[slot, way],
            x_recv.at[slot, way],
            device_id={"tp": partner},
            device_id_type=MESH,
        )

    def far_ref(slot, way, chip):
        return recv.at[slot, core, chip, pl.ds(way * piece, piece)]

    def far_copy(slot, way):
        came = lax.rem(x + (n_x - 1 if way == 0 else 1), n_x)
        to = lax.rem(x + (1 if way == 0 else n_x - 1), n_x) * cores + core
        return pltpu.make_async_remote_copy(
            far_ref(slot, way, came),
            far_ref(slot, way, came),
            far_send.at[slot, way],
            far_recv.at[slot, way],
            device_id={"tp": to},
            device_id_type=MESH,
        )

    def far_arrival(slot, way):
        came = lax.rem(x + 2, n_x)
        return pltpu.make_async_remote_copy(
            far_ref(slot, way, came),
            far_ref(slot, way, came),
            far_send.at[slot, way],
            far_recv.at[slot, way],
            device_id={"tp": partner},
            device_id_type=MESH,
        )

    def p_copy(slot):
        return pltpu.make_async_remote_copy(
            recv.at[slot, core], recv.at[slot, core], p_send.at[slot], p_recv.at[slot],
            device_id={"tp": partner}, device_id_type=MESH,
        )

    def p_arrival(slot):
        return pltpu.make_async_remote_copy(
            recv.at[slot, 1 - core], recv.at[slot, 1 - core], p_send.at[slot], p_recv.at[slot],
            device_id={"tp": partner}, device_id_type=MESH,
        )

    def part_copy():
        return pltpu.make_async_remote_copy(
            parts.at[rank], parts.at[rank], part_send, part_recv,
            device_id={"sp": at_rank(0)}, device_id_type=MESH,
        )

    def result_copy(r):
        return pltpu.make_async_remote_copy(
            result, result, result_send.at[r], result_recv, device_id={"sp": at_rank(r)}, device_id_type=MESH
        )

    for load in loads:
        load.wait()

    def send(q):
        z_copy(q).start()
        bias_copy(q).start()

    def answer(r, carry):
        first = jnp.where(r == 0, late, jnp.where(r <= late, r - 1, r))
        send(rank - jnp.where(rank > late, first, r))
        return carry

    lax.fori_loop(0, jnp.minimum(rank, FIRST), answer, 0)
    out_row, in_row = iota((4 * 2 * piece, 4 * 2 * piece), 0), iota((4 * 2 * piece, 4 * 2 * piece), 1)
    source = (
        lax.rem(out_row, 2) * (4 * piece)
        + lax.rem(lax.div(out_row, 2), 2) * (2 * piece)
        + lax.div(out_row, 4)
    )
    perm[...] = jnp.where(in_row == source, 1.0, 0.0).astype(BF16)
    later_mask[...] = jnp.where(iota((rows, rows), 0) > iota((rows, rows), 1), 1.0, 0.0).astype(BF16)

    gains = gain_v[...].astype(F32)
    for t in range(cores * n_x):
        gain_f[t] = jnp.concatenate(
            [gains[t * feat // LANES + j : t * feat // LANES + j + 1] for j in range(feat // LANES)], axis=1
        )
    queries = query_v[...].astype(F32)
    for s in range(seqs):
        query_f[s] = queries[s : s + 1]

    def project(piece_of, count):
        squares = jnp.zeros((count, feat), F32)
        for t in range(cores * n_x):
            value = piece_of(t).astype(F32)
            squares = squares + value * value
        inverse = lax.rsqrt(jnp.sum(squares, axis=1, keepdims=True) / width + norm_eps)
        for t in range(cores * n_x):
            value = piece_of(t).astype(F32) * inverse * gain_f[t]
            normed[pl.ds(0, count), pl.ds(t * feat, feat)] = value.astype(BF16)
        return jnp.dot(normed[pl.ds(0, count), :], weight_v[...], preferred_element_type=F32).astype(BF16)

    lane = iota((1, LANES), 1)

    def own_read(s, totals):
        projected = project(
            lambda t: tok_v[pl.ds(s * span, span), :, pl.ds(t * feat, feat)].reshape(rows, feat), rows
        )
        keys, values = projected[:, :columns], projected[:, columns:]
        head_row, head_lane = iota((8, columns), 0), lax.div(iota((8, columns), 1), head_size)
        spread = jnp.where(head_row == head_lane, query_f[s], 0.0).astype(BF16)
        logits = lax.dot_general(spread, keys, (((1,), (1,)), ((), ())), preferred_element_type=F32)
        terms = jnp.concatenate([bias_v[s].astype(F32), jnp.zeros((8 - heads, rows), F32)], axis=0)
        logits = logits * head_size ** (-0.5) + terms
        soft = jnp.log1p(jnp.exp(-jnp.abs(logits)))
        keep = jnp.minimum(-logits, 0.0) - soft
        take = jnp.minimum(logits, 0.0) - soft
        high = keep.astype(BF16).astype(F32)
        middle = (keep - high).astype(BF16).astype(F32)
        low = keep - high - middle
        split = jnp.concatenate([high, middle, low, jnp.zeros_like(low)], axis=0).astype(BF16)
        sums = jnp.dot(split, later_mask[...], preferred_element_type=F32)
        later = sums[0:8] + sums[8:16] + sums[16:24]
        weights = jnp.exp(take + later)
        high = weights.astype(BF16).astype(F32)
        split = jnp.concatenate([high, weights - high], axis=0).astype(BF16)
        mixed = jnp.dot(split, values, preferred_element_type=F32)
        mixed = mixed[0:8] + mixed[8:16]
        read = jnp.sum(jnp.where(head_row == head_lane, mixed, 0.0), axis=0, keepdims=True)
        parts[rank, :, pl.ds(pl.multiple_of(s * columns, columns), columns)] = read
        total = jnp.sum(keep, axis=1, keepdims=True)
        for h in range(heads):
            totals = totals + jnp.where(lane == s * heads + h, total[h : h + 1], 0.0)
        return totals

    own_tile = lax.div(lax.rem(z, span), per_tile)
    own_bias = pltpu.make_async_copy(
        bias.at[lax.div(z, span), :, pl.ds(pl.multiple_of(own_tile * LANES, LANES), LANES)],
        bias_recv.at[z],
        bias_own_sem,
    )
    own_bias.start()
    own.wait()

    parts[rank, :, pl.ds(blocks * LANES, LANES)] = lax.fori_loop(0, seqs, own_read, jnp.zeros((1, LANES), F32))

    @pl.when(rank > 0)
    def _():
        part_copy().start()

    lax.fori_loop(jnp.minimum(rank, FIRST), rank, answer, 0)

    def higher(q):
        @pl.when((q > rank) & (q < n))
        def _():
            pl.semaphore_wait(ready.at[q], 1)
            send(q)

    def step(k, carry):
        @pl.when(k >= P_LAG)
        def _():
            slot = k - P_LAG
            p_arrival(slot).wait_recv()
            projected = project(lambda t: recv[slot, t % cores, t // cores], 2 * piece)
            stacked = jnp.concatenate(
                [projected[:, j * LANES : (j + 1) * LANES] for j in range(2 * columns // LANES)], axis=0
            )
            placed = jnp.dot(perm[...], stacked, preferred_element_type=F32).astype(BF16)
            for half in range(2):
                q = 2 * slot + half
                at = at_rank(jnp.where(q <= rank, rank - q, q))
                cache_out[pl.ds(pl.multiple_of(at * 4 * piece, 4 * piece), 4 * piece)] = placed[
                    half * 4 * piece : (half + 1) * 4 * piece
                ]

        @pl.when((k >= FAR_LAG) & (k < steps + FAR_LAG))
        def _():
            slot = k - FAR_LAG
            for way in range(2):
                far_arrival(slot, way).wait_recv()
            p_copy(slot).start()

        @pl.when((k >= X_LAG) & (k < steps + X_LAG))
        def _():
            slot = k - X_LAG
            for way in range(2):
                x_arrival(slot, way).wait_recv()
                far_copy(slot, way).start()

        @pl.when((k >= Z_LAG) & (k < steps + Z_LAG))
        def _():
            slot = k - Z_LAG

            @pl.when(slot > 0)
            def _():
                z_arrival(2 * slot).wait_recv()

            z_arrival(2 * slot + 1).wait_recv()
            for way in range(2):
                x_copy(slot, way).start()

        higher(rank + 1 + 2 * k)
        higher(rank + 2 + 2 * k)
        return carry

    lax.fori_loop(0, steps + P_LAG, step, 0)

    @pl.when(rank == 0)
    def _():
        others = parts.at[pl.ds(1, n - 1)]
        pltpu.make_async_copy(others, others, part_recv).wait()
        by_position = [parts[late if j == 0 else j - 1 if j <= late else j] for j in range(n)]
        result[...] = stick(by_position, blocks, seqs)[0]

        def tell(r, carry):
            result_copy(r).start()
            return carry

        lax.fori_loop(1, n, tell, 0)

    own_bias.wait()
    others = pl.ds(0, n - 1)
    pltpu.make_async_copy(bias_recv.at[others], bias_recv.at[others], b_recv).wait()
    arrived = bias_recv[...].astype(F32)
    part = lax.rem(lax.rem(z, span), per_tile)
    chosen = arrived[:, :, 0:piece]
    for j in range(1, per_tile):
        chosen = jnp.where(part == j, arrived[:, :, j * piece : (j + 1) * piece], chosen)
    bias_out[...] = chosen.astype(BF16)

    @pl.when(rank > 0)
    def _():
        result_copy(0).wait_recv()

    for s in range(seqs):
        att_out[pl.ds(s, 1), :] = result[:, s * columns : (s + 1) * columns]

    pltpu.make_async_copy(bias_recv.at[others], bias_recv.at[others], b_send).wait()

    @pl.when(rank > 0)
    def _():
        part_copy().wait_send()

    @pl.when(rank == 0)
    def _():
        def told(r, carry):
            result_copy(r).wait_send()
            return carry

        lax.fori_loop(1, n, told, 0)

    def drain(slot, carry):
        for way in range(2):
            x_copy(slot, way).wait_send()
            far_copy(slot, way).wait_send()
        p_copy(slot).wait_send()

        @pl.when(slot > 0)
        def _():
            z_copy(2 * slot).wait_send()

        z_copy(2 * slot + 1).wait_send()
        return carry

    lax.fori_loop(0, steps, drain, 0)


def local(cores, tokens, norm_gain, key_weight, value_weight, break_bias, new_query):
    seqs, tok_rows, width = tokens.shape
    heads = break_bias.shape[2]
    columns = key_weight.shape[1]
    n = lax.axis_size("sp")
    n_tp = lax.axis_size("tp")
    n_x = n_tp // cores
    piece = tok_rows * seqs // n
    span = n // seqs
    steps = n // 2
    feat = width // n_tp
    shape = (n, cores, n_x, piece, seqs, heads, width, columns)
    dma = pltpu.SemaphoreType.DMA
    message = seqs * columns + LANES
    cache, bias_out, attended = pl.pallas_call(
        functools.partial(kernel, shape),
        out_shape=(
            jax.ShapeDtypeStruct((n * piece * 4, LANES), BF16),
            jax.ShapeDtypeStruct((n, heads, piece), BF16),
            jax.ShapeDtypeStruct((seqs, columns), F32),
        ),
        in_specs=[pl.BlockSpec(memory_space=pltpu.HBM)] * 6,
        out_specs=[pl.BlockSpec(memory_space=pltpu.VMEM)] * 3,
        scratch_shapes=[
            pltpu.VMEM((n, piece, width), BF16),
            pltpu.VMEM((width, 2 * columns), BF16),
            pltpu.VMEM((steps, cores, n_x, 2 * piece, feat), BF16),
            pltpu.VMEM((max(span, 2) * piece, width), BF16),
            pltpu.VMEM((seqs, heads, tok_rows), BF16),
            pltpu.VMEM((n, heads, LANES), BF16),
            pltpu.VMEM((seqs, columns), BF16),
            pltpu.VMEM((seqs, 1, columns), F32),
            pltpu.VMEM((width // LANES, LANES), BF16),
            pltpu.VMEM((n_tp, 1, feat), F32),
            pltpu.VMEM((8 * piece, 8 * piece), BF16),
            pltpu.VMEM((tok_rows, tok_rows), BF16),
            pltpu.VMEM((n, 1, message), F32),
            pltpu.VMEM((1, seqs * columns), F32),
            pltpu.SemaphoreType.REGULAR((n,)),
            dma((6,)),
            dma,
            dma,
            dma((n,)),
            dma((n,)),
            dma,
            dma,
            dma((steps, 2)),
            dma((steps, 2)),
            dma((steps, 2)),
            dma((steps, 2)),
            dma((steps,)),
            dma((steps,)),
            dma,
            dma,
            dma((n,)),
            dma,
        ],
        compiler_params=pltpu.CompilerParams(
            collective_id=0, has_side_effects=True, vmem_limit_bytes=48 * 1024 * 1024
        ),
    )(
        *(
            pltpu.with_memory_space_constraint(array, pltpu.HBM)
            for array in (
                tokens.reshape(n, piece, width),
                norm_gain.reshape(width // LANES, LANES),
                key_weight,
                value_weight,
                jnp.transpose(break_bias, (0, 2, 1)),
                new_query,
            )
        )
    )
    halves = columns // LANES
    paired = cache.reshape(n, piece, halves, 2, LANES)
    paired = jnp.transpose(paired, (0, 1, 3, 2, 4)).reshape(n, piece, 2, columns)
    return (paired[None], jnp.transpose(bias_out, (0, 2, 1))[None], attended)


def solution(mesh):
    return jax.shard_map(
        functools.partial(local, 2),
        mesh=mesh,
        in_specs=(
            P("grp", "sp", None),
            P(),
            P(None, "tp"),
            P(None, "tp"),
            P("grp", "sp", "tp"),
            P("grp", "tp"),
        ),
        out_specs=(
            P(("grp", "sp"), None, None, None, "tp"),
            P(("grp", "sp"), None, None, "tp"),
            P("grp", "tp"),
        ),
        check_vma=False,
    )
```

```python
import functools

import jax
import jax.numpy as jnp
from jax import lax
from jax.experimental import pallas as pl
from jax.experimental.pallas import tpu as pltpu
from jax.sharding import PartitionSpec as P

norm_eps = 1e-06
LANES = 128
MESH = pl.DeviceIdType.MESH
F32 = jnp.float32
BF16 = jnp.bfloat16
Z_LAG, X_LAG, FAR_LAG, P_LAG = 4, 7, 10, 13
FIRST = 10


def iota(shape, axis):
    return lax.broadcasted_iota(jnp.int32, shape, axis)


def stick(rows, blocks, seqs_heads):
    carry = jnp.zeros((1, LANES), F32)
    carries = [carry]
    for row in rows[:0:-1]:
        carry = carry + row[:, blocks * LANES :]
        carries.append(carry)
    total = carry + rows[0][:, blocks * LANES :]
    factors = jnp.exp(jnp.concatenate(carries[::-1], axis=0))
    stacked = jnp.concatenate([row[:, : blocks * LANES] for row in rows], axis=0)
    parts = []
    for block in range(blocks):
        mine = stacked[:, block * LANES : (block + 1) * LANES] * factors[:, block : block + 1]
        parts.append(jnp.sum(mine, axis=0, keepdims=True))
    return jnp.concatenate(parts, axis=1), total


def kernel(
    shape,
    tokens,
    gain,
    key_weight,
    value_weight,
    bias,
    query,
    cache_out,
    bias_out,
    att_out,
    tok_v,
    weight_v,
    recv,
    normed,
    bias_v,
    bias_recv,
    query_v,
    query_f,
    gain_v,
    gain_f,
    perm,
    later_mask,
    parts,
    result,
    ready,
    load_sem,
    own_sem,
    bias_own_sem,
    z_send,
    z_recv,
    b_send,
    b_recv,
    x_send,
    x_recv,
    far_send,
    far_recv,
    p_send,
    p_recv,
    part_send,
    part_recv,
    result_send,
    result_recv,
):
    n, cores, n_x, piece, seqs, heads, width, columns = shape
    steps = n // 2
    span = n // seqs
    rows = span * piece
    feat = width // (cores * n_x)
    head_size = columns // heads
    blocks = seqs * heads
    per_tile = LANES // piece
    z = lax.axis_index("sp")
    tp = lax.axis_index("tp")
    core = lax.rem(tp, cores)
    x = lax.div(tp, cores)
    partner = x * cores + (1 - core)
    mine = pl.ds(pl.multiple_of(tp * feat, feat), feat)

    late = n // 4
    rank = jnp.where(z == 0, late, jnp.where(z <= late, z - 1, z))

    def at_rank(r):
        return jnp.where(r == late, 0, jnp.where(r < late, r + 1, r))

    barrier = pltpu.get_barrier_semaphore()

    def greet(higher, carry):
        pl.semaphore_signal(barrier, 1, device_id={"sp": at_rank(higher)}, device_id_type=MESH)
        return carry

    lax.fori_loop(rank + 1, n, greet, 0)
    for offset in range(1, n_x):
        pl.semaphore_signal(
            barrier, 1, device_id={"tp": lax.rem(x + offset, n_x) * cores + core}, device_id_type=MESH
        )
    pl.semaphore_signal(barrier, 1, device_id={"tp": partner}, device_id_type=MESH)

    loads = [
        pltpu.make_async_copy(gain, gain_v, load_sem.at[0]),
        pltpu.make_async_copy(bias, bias_v, load_sem.at[1]),
        pltpu.make_async_copy(query, query_v, load_sem.at[2]),
        pltpu.make_async_copy(tokens, tok_v, load_sem.at[3]),
        pltpu.make_async_copy(key_weight, weight_v.at[:, pl.ds(0, columns)], load_sem.at[4]),
        pltpu.make_async_copy(value_weight, weight_v.at[:, pl.ds(columns, columns)], load_sem.at[5]),
    ]
    for load in loads:
        load.start()
    own = pltpu.make_async_copy(tokens.at[z, :, mine], recv.at[0, core, x, pl.ds(0, piece)], own_sem)
    own.start()

    pl.semaphore_wait(barrier, rank + n_x)

    def report(q, carry):
        pl.semaphore_signal(ready.at[rank], 1, device_id={"sp": at_rank(rank - q)}, device_id_type=MESH)
        return carry

    lax.fori_loop(1, rank + 1, report, 0)

    def z_copy(q):
        lower = q <= rank
        peer = jnp.where(lower, rank - q, q)
        slot = jnp.where(lower, rank, q - rank)
        to = at_rank(peer)
        return pltpu.make_async_remote_copy(
            tok_v.at[to, :, mine],
            recv.at[lax.div(slot, 2), core, x, pl.ds(pl.multiple_of(lax.rem(slot, 2) * piece, piece), piece)],
            z_send.at[q],
            z_recv.at[slot],
            device_id={"sp": to},
            device_id_type=MESH,
        )

    def z_arrival(q):
        return pltpu.make_async_remote_copy(
            tok_v.at[z, :, mine],
            recv.at[lax.div(q, 2), core, x, pl.ds(pl.multiple_of(lax.rem(q, 2) * piece, piece), piece)],
            z_send.at[q],
            z_recv.at[q],
            device_id={"sp": z},
            device_id_type=MESH,
        )

    def bias_copy(q):
        to = at_rank(jnp.where(q <= rank, rank - q, q))
        tile = lax.div(lax.rem(to, span), per_tile)
        return pltpu.make_async_remote_copy(
            bias_v.at[lax.div(to, span), :, pl.ds(pl.multiple_of(tile * LANES, LANES), LANES)],
            bias_recv.at[z],
            b_send,
            b_recv,
            device_id={"sp": to},
            device_id_type=MESH,
        )

    def x_copy(slot, way):
        to = lax.rem(x + (1 if way == 0 else n_x - 1), n_x) * cores + core
        return pltpu.make_async_remote_copy(
            recv.at[slot, core, x],
            recv.at[slot, core, x],
            x_send.at[slot, way],
            x_recv.at[slot, way],
            device_id={"tp": to},
            device_id_type=MESH,
        )

    def x_arrival(slot, way):
        came = lax.rem(x + (n_x - 1 if way == 0 else 1), n_x)
        return pltpu.make_async_remote_copy(
            recv.at[slot, core, came],
            recv.at[slot, core, came],
            x_send.at[slot, way],
            x_recv.at[slot, way],
            device_id={"tp": partner},
            device_id_type=MESH,
        )

    def far_ref(slot, way, chip):
        return recv.at[slot, core, chip, pl.ds(way * piece, piece)]

    def far_copy(slot, way):
        came = lax.rem(x + (n_x - 1 if way == 0 else 1), n_x)
        to = lax.rem(x + (1 if way == 0 else n_x - 1), n_x) * cores + core
        return pltpu.make_async_remote_copy(
            far_ref(slot, way, came),
            far_ref(slot, way, came),
            far_send.at[slot, way],
            far_recv.at[slot, way],
            device_id={"tp": to},
            device_id_type=MESH,
        )

    def far_arrival(slot, way):
        came = lax.rem(x + 2, n_x)
        return pltpu.make_async_remote_copy(
            far_ref(slot, way, came),
            far_ref(slot, way, came),
            far_send.at[slot, way],
            far_recv.at[slot, way],
            device_id={"tp": partner},
            device_id_type=MESH,
        )

    def p_copy(slot):
        return pltpu.make_async_remote_copy(
            recv.at[slot, core], recv.at[slot, core], p_send.at[slot], p_recv.at[slot],
            device_id={"tp": partner}, device_id_type=MESH,
        )

    def p_arrival(slot):
        return pltpu.make_async_remote_copy(
            recv.at[slot, 1 - core], recv.at[slot, 1 - core], p_send.at[slot], p_recv.at[slot],
            device_id={"tp": partner}, device_id_type=MESH,
        )

    def part_copy():
        return pltpu.make_async_remote_copy(
            parts.at[rank], parts.at[rank], part_send, part_recv,
            device_id={"sp": at_rank(0)}, device_id_type=MESH,
        )

    def result_copy(r):
        return pltpu.make_async_remote_copy(
            result, result, result_send.at[r], result_recv, device_id={"sp": at_rank(r)}, device_id_type=MESH
        )

    for load in loads:
        load.wait()

    def send(q):
        z_copy(q).start()
        bias_copy(q).start()

    def answer(r, carry):
        first = jnp.where(r == 0, late, jnp.where(r <= late, r - 1, r))
        send(rank - jnp.where(rank > late, first, r))
        return carry

    lax.fori_loop(0, jnp.minimum(rank, FIRST), answer, 0)
    out_row, in_row = iota((4 * 2 * piece, 4 * 2 * piece), 0), iota((4 * 2 * piece, 4 * 2 * piece), 1)
    source = (
        lax.rem(out_row, 2) * (4 * piece)
        + lax.rem(lax.div(out_row, 2), 2) * (2 * piece)
        + lax.div(out_row, 4)
    )
    perm[...] = jnp.where(in_row == source, 1.0, 0.0).astype(BF16)
    later_mask[...] = jnp.where(iota((rows, rows), 0) > iota((rows, rows), 1), 1.0, 0.0).astype(BF16)

    gains = gain_v[...].astype(F32)
    for t in range(cores * n_x):
        gain_f[t] = jnp.concatenate(
            [gains[t * feat // LANES + j : t * feat // LANES + j + 1] for j in range(feat // LANES)], axis=1
        )
    queries = query_v[...].astype(F32)
    for s in range(seqs):
        query_f[s] = queries[s : s + 1]

    def project(piece_of, count):
        squares = jnp.zeros((count, feat), F32)
        for t in range(cores * n_x):
            value = piece_of(t).astype(F32)
            squares = squares + value * value
        inverse = lax.rsqrt(jnp.sum(squares, axis=1, keepdims=True) / width + norm_eps)
        for t in range(cores * n_x):
            value = piece_of(t).astype(F32) * inverse * gain_f[t]
            normed[pl.ds(0, count), pl.ds(t * feat, feat)] = value.astype(BF16)
        return jnp.dot(normed[pl.ds(0, count), :], weight_v[...], preferred_element_type=F32).astype(BF16)

    lane = iota((1, LANES), 1)

    def own_read(s, totals):
        projected = project(
            lambda t: tok_v[pl.ds(s * span, span), :, pl.ds(t * feat, feat)].reshape(rows, feat), rows
        )
        keys, values = projected[:, :columns], projected[:, columns:]
        head_row, head_lane = iota((8, columns), 0), lax.div(iota((8, columns), 1), head_size)
        spread = jnp.where(head_row == head_lane, query_f[s], 0.0).astype(BF16)
        logits = lax.dot_general(spread, keys, (((1,), (1,)), ((), ())), preferred_element_type=F32)
        terms = jnp.concatenate([bias_v[s].astype(F32), jnp.zeros((8 - heads, rows), F32)], axis=0)
        logits = logits * head_size ** (-0.5) + terms
        soft = jnp.log1p(jnp.exp(-jnp.abs(logits)))
        keep = jnp.minimum(-logits, 0.0) - soft
        take = jnp.minimum(logits, 0.0) - soft
        high = keep.astype(BF16).astype(F32)
        middle = (keep - high).astype(BF16).astype(F32)
        low = keep - high - middle
        split = jnp.concatenate([high, middle, low, jnp.zeros_like(low)], axis=0).astype(BF16)
        sums = jnp.dot(split, later_mask[...], preferred_element_type=F32)
        later = sums[0:8] + sums[8:16] + sums[16:24]
        weights = jnp.exp(take + later)
        high = weights.astype(BF16).astype(F32)
        split = jnp.concatenate([high, weights - high], axis=0).astype(BF16)
        mixed = jnp.dot(split, values, preferred_element_type=F32)
        mixed = mixed[0:8] + mixed[8:16]
        read = jnp.sum(jnp.where(head_row == head_lane, mixed, 0.0), axis=0, keepdims=True)
        parts[rank, :, pl.ds(pl.multiple_of(s * columns, columns), columns)] = read
        total = jnp.sum(keep, axis=1, keepdims=True)
        for h in range(heads):
            totals = totals + jnp.where(lane == s * heads + h, total[h : h + 1], 0.0)
        return totals

    own_tile = lax.div(lax.rem(z, span), per_tile)
    own_bias = pltpu.make_async_copy(
        bias.at[lax.div(z, span), :, pl.ds(pl.multiple_of(own_tile * LANES, LANES), LANES)],
        bias_recv.at[z],
        bias_own_sem,
    )
    own_bias.start()
    own.wait()

    parts[rank, :, pl.ds(blocks * LANES, LANES)] = lax.fori_loop(0, seqs, own_read, jnp.zeros((1, LANES), F32))

    @pl.when(rank > 0)
    def _():
        part_copy().start()

    lax.fori_loop(jnp.minimum(rank, FIRST), rank, answer, 0)

    def higher(q):
        @pl.when((q > rank) & (q < n))
        def _():
            pl.semaphore_wait(ready.at[q], 1)
            send(q)

    def step(k, carry):
        @pl.when(k >= P_LAG)
        def _():
            slot = k - P_LAG
            p_arrival(slot).wait_recv()
            projected = project(lambda t: recv[slot, t % cores, t // cores], 2 * piece)
            stacked = jnp.concatenate(
                [projected[:, j * LANES : (j + 1) * LANES] for j in range(2 * columns // LANES)], axis=0
            )
            placed = jnp.dot(perm[...], stacked, preferred_element_type=F32).astype(BF16)
            for half in range(2):
                q = 2 * slot + half
                at = at_rank(jnp.where(q <= rank, rank - q, q))
                cache_out[pl.ds(pl.multiple_of(at * 4 * piece, 4 * piece), 4 * piece)] = placed[
                    half * 4 * piece : (half + 1) * 4 * piece
                ]

        @pl.when((k >= FAR_LAG) & (k < steps + FAR_LAG))
        def _():
            slot = k - FAR_LAG
            for way in range(2):
                far_arrival(slot, way).wait_recv()
            p_copy(slot).start()

        @pl.when((k >= X_LAG) & (k < steps + X_LAG))
        def _():
            slot = k - X_LAG
            for way in range(2):
                x_arrival(slot, way).wait_recv()
                far_copy(slot, way).start()

        @pl.when((k >= Z_LAG) & (k < steps + Z_LAG))
        def _():
            slot = k - Z_LAG

            @pl.when(slot > 0)
            def _():
                z_arrival(2 * slot).wait_recv()

            z_arrival(2 * slot + 1).wait_recv()
            for way in range(2):
                x_copy(slot, way).start()

        higher(rank + 1 + 2 * k)
        higher(rank + 2 + 2 * k)

        @pl.when((rank == 0) & (k == steps + Z_LAG))
        def _():
            others = parts.at[pl.ds(1, n - 1)]
            pltpu.make_async_copy(others, others, part_recv).wait()
            by_position = [parts[late if j == 0 else j - 1 if j <= late else j] for j in range(n)]
            result[...] = stick(by_position, blocks, seqs)[0]

            def tell(r, carry):
                result_copy(r).start()
                return carry

            lax.fori_loop(1, n, tell, 0)

        return carry

    lax.fori_loop(0, steps + P_LAG, step, 0)

    own_bias.wait()
    others = pl.ds(0, n - 1)
    pltpu.make_async_copy(bias_recv.at[others], bias_recv.at[others], b_recv).wait()
    arrived = bias_recv[...].astype(F32)
    part = lax.rem(lax.rem(z, span), per_tile)
    chosen = arrived[:, :, 0:piece]
    for j in range(1, per_tile):
        chosen = jnp.where(part == j, arrived[:, :, j * piece : (j + 1) * piece], chosen)
    bias_out[...] = chosen.astype(BF16)

    @pl.when(rank > 0)
    def _():
        result_copy(0).wait_recv()

    for s in range(seqs):
        att_out[pl.ds(s, 1), :] = result[:, s * columns : (s + 1) * columns]

    pltpu.make_async_copy(bias_recv.at[others], bias_recv.at[others], b_send).wait()

    @pl.when(rank > 0)
    def _():
        part_copy().wait_send()

    @pl.when(rank == 0)
    def _():
        def told(r, carry):
            result_copy(r).wait_send()
            return carry

        lax.fori_loop(1, n, told, 0)

    def drain(slot, carry):
        for way in range(2):
            x_copy(slot, way).wait_send()
            far_copy(slot, way).wait_send()
        p_copy(slot).wait_send()

        @pl.when(slot > 0)
        def _():
            z_copy(2 * slot).wait_send()

        z_copy(2 * slot + 1).wait_send()
        return carry

    lax.fori_loop(0, steps, drain, 0)


def local(cores, tokens, norm_gain, key_weight, value_weight, break_bias, new_query):
    seqs, tok_rows, width = tokens.shape
    heads = break_bias.shape[2]
    columns = key_weight.shape[1]
    n = lax.axis_size("sp")
    n_tp = lax.axis_size("tp")
    n_x = n_tp // cores
    piece = tok_rows * seqs // n
    span = n // seqs
    steps = n // 2
    feat = width // n_tp
    shape = (n, cores, n_x, piece, seqs, heads, width, columns)
    dma = pltpu.SemaphoreType.DMA
    message = seqs * columns + LANES
    cache, bias_out, attended = pl.pallas_call(
        functools.partial(kernel, shape),
        out_shape=(
            jax.ShapeDtypeStruct((n * piece * 4, LANES), BF16),
            jax.ShapeDtypeStruct((n, heads, piece), BF16),
            jax.ShapeDtypeStruct((seqs, columns), F32),
        ),
        in_specs=[pl.BlockSpec(memory_space=pltpu.HBM)] * 6,
        out_specs=[pl.BlockSpec(memory_space=pltpu.VMEM)] * 3,
        scratch_shapes=[
            pltpu.VMEM((n, piece, width), BF16),
            pltpu.VMEM((width, 2 * columns), BF16),
            pltpu.VMEM((steps, cores, n_x, 2 * piece, feat), BF16),
            pltpu.VMEM((max(span, 2) * piece, width), BF16),
            pltpu.VMEM((seqs, heads, tok_rows), BF16),
            pltpu.VMEM((n, heads, LANES), BF16),
            pltpu.VMEM((seqs, columns), BF16),
            pltpu.VMEM((seqs, 1, columns), F32),
            pltpu.VMEM((width // LANES, LANES), BF16),
            pltpu.VMEM((n_tp, 1, feat), F32),
            pltpu.VMEM((8 * piece, 8 * piece), BF16),
            pltpu.VMEM((tok_rows, tok_rows), BF16),
            pltpu.VMEM((n, 1, message), F32),
            pltpu.VMEM((1, seqs * columns), F32),
            pltpu.SemaphoreType.REGULAR((n,)),
            dma((6,)),
            dma,
            dma,
            dma((n,)),
            dma((n,)),
            dma,
            dma,
            dma((steps, 2)),
            dma((steps, 2)),
            dma((steps, 2)),
            dma((steps, 2)),
            dma((steps,)),
            dma((steps,)),
            dma,
            dma,
            dma((n,)),
            dma,
        ],
        compiler_params=pltpu.CompilerParams(
            collective_id=0, has_side_effects=True, vmem_limit_bytes=48 * 1024 * 1024
        ),
    )(
        *(
            pltpu.with_memory_space_constraint(array, pltpu.HBM)
            for array in (
                tokens.reshape(n, piece, width),
                norm_gain.reshape(width // LANES, LANES),
                key_weight,
                value_weight,
                jnp.transpose(break_bias, (0, 2, 1)),
                new_query,
            )
        )
    )
    halves = columns // LANES
    paired = cache.reshape(n, piece, halves, 2, LANES)
    paired = jnp.transpose(paired, (0, 1, 3, 2, 4)).reshape(n, piece, 2, columns)
    return (paired[None], jnp.transpose(bias_out, (0, 2, 1))[None], attended)


def solution(mesh):
    return jax.shard_map(
        functools.partial(local, 2),
        mesh=mesh,
        in_specs=(
            P("grp", "sp", None),
            P(),
            P(None, "tp"),
            P(None, "tp"),
            P("grp", "sp", "tp"),
            P("grp", "tp"),
        ),
        out_specs=(
            P(("grp", "sp"), None, None, None, "tp"),
            P(("grp", "sp"), None, None, "tp"),
            P("grp", "tp"),
        ),
        check_vma=False,
    )
```

```python
import functools

import jax
import jax.numpy as jnp
from jax import lax
from jax.experimental import pallas as pl
from jax.experimental.pallas import tpu as pltpu
from jax.sharding import PartitionSpec as P

norm_eps = 1e-06
LANES = 128
MESH = pl.DeviceIdType.MESH
F32 = jnp.float32
BF16 = jnp.bfloat16
Z_LAG, X_LAG, FAR_LAG, P_LAG = 4, 7, 10, 13
FIRST = 16


def iota(shape, axis):
    return lax.broadcasted_iota(jnp.int32, shape, axis)


def stick(rows, blocks, seqs_heads):
    carry = jnp.zeros((1, LANES), F32)
    carries = [carry]
    for row in rows[:0:-1]:
        carry = carry + row[:, blocks * LANES :]
        carries.append(carry)
    total = carry + rows[0][:, blocks * LANES :]
    factors = jnp.exp(jnp.concatenate(carries[::-1], axis=0))
    stacked = jnp.concatenate([row[:, : blocks * LANES] for row in rows], axis=0)
    parts = []
    for block in range(blocks):
        mine = stacked[:, block * LANES : (block + 1) * LANES] * factors[:, block : block + 1]
        parts.append(jnp.sum(mine, axis=0, keepdims=True))
    return jnp.concatenate(parts, axis=1), total


def kernel(
    shape,
    tokens,
    gain,
    key_weight,
    value_weight,
    bias,
    query,
    cache_out,
    bias_out,
    att_out,
    tok_v,
    weight_v,
    recv,
    normed,
    bias_v,
    bias_recv,
    query_v,
    query_f,
    gain_v,
    gain_f,
    perm,
    later_mask,
    parts,
    result,
    ready,
    load_sem,
    own_sem,
    bias_own_sem,
    z_send,
    z_recv,
    b_send,
    b_recv,
    x_send,
    x_recv,
    far_send,
    far_recv,
    p_send,
    p_recv,
    part_send,
    part_recv,
    result_send,
    result_recv,
):
    n, cores, n_x, piece, seqs, heads, width, columns = shape
    steps = n // 2
    span = n // seqs
    rows = span * piece
    feat = width // (cores * n_x)
    head_size = columns // heads
    blocks = seqs * heads
    per_tile = LANES // piece
    z = lax.axis_index("sp")
    tp = lax.axis_index("tp")
    core = lax.rem(tp, cores)
    x = lax.div(tp, cores)
    partner = x * cores + (1 - core)
    mine = pl.ds(pl.multiple_of(tp * feat, feat), feat)

    late = n // 4
    rank = jnp.where(z == 0, late, jnp.where(z <= late, z - 1, z))

    def at_rank(r):
        return jnp.where(r == late, 0, jnp.where(r < late, r + 1, r))

    barrier = pltpu.get_barrier_semaphore()

    def greet(higher, carry):
        pl.semaphore_signal(barrier, 1, device_id={"sp": at_rank(higher)}, device_id_type=MESH)
        return carry

    lax.fori_loop(rank + 1, n, greet, 0)
    for offset in range(1, n_x):
        pl.semaphore_signal(
            barrier, 1, device_id={"tp": lax.rem(x + offset, n_x) * cores + core}, device_id_type=MESH
        )
    pl.semaphore_signal(barrier, 1, device_id={"tp": partner}, device_id_type=MESH)

    loads = [
        pltpu.make_async_copy(gain, gain_v, load_sem.at[0]),
        pltpu.make_async_copy(bias, bias_v, load_sem.at[1]),
        pltpu.make_async_copy(query, query_v, load_sem.at[2]),
        pltpu.make_async_copy(tokens, tok_v, load_sem.at[3]),
        pltpu.make_async_copy(key_weight, weight_v.at[:, pl.ds(0, columns)], load_sem.at[4]),
        pltpu.make_async_copy(value_weight, weight_v.at[:, pl.ds(columns, columns)], load_sem.at[5]),
    ]
    for load in loads:
        load.start()
    own = pltpu.make_async_copy(tokens.at[z, :, mine], recv.at[0, core, x, pl.ds(0, piece)], own_sem)
    own.start()

    pl.semaphore_wait(barrier, rank + n_x)

    def report(q, carry):
        pl.semaphore_signal(ready.at[rank], 1, device_id={"sp": at_rank(rank - q)}, device_id_type=MESH)
        return carry

    lax.fori_loop(1, rank + 1, report, 0)

    def z_copy(q):
        lower = q <= rank
        peer = jnp.where(lower, rank - q, q)
        slot = jnp.where(lower, rank, q - rank)
        to = at_rank(peer)
        return pltpu.make_async_remote_copy(
            tok_v.at[to, :, mine],
            recv.at[lax.div(slot, 2), core, x, pl.ds(pl.multiple_of(lax.rem(slot, 2) * piece, piece), piece)],
            z_send.at[q],
            z_recv.at[slot],
            device_id={"sp": to},
            device_id_type=MESH,
        )

    def z_arrival(q):
        return pltpu.make_async_remote_copy(
            tok_v.at[z, :, mine],
            recv.at[lax.div(q, 2), core, x, pl.ds(pl.multiple_of(lax.rem(q, 2) * piece, piece), piece)],
            z_send.at[q],
            z_recv.at[q],
            device_id={"sp": z},
            device_id_type=MESH,
        )

    def bias_copy(q):
        to = at_rank(jnp.where(q <= rank, rank - q, q))
        tile = lax.div(lax.rem(to, span), per_tile)
        return pltpu.make_async_remote_copy(
            bias_v.at[lax.div(to, span), :, pl.ds(pl.multiple_of(tile * LANES, LANES), LANES)],
            bias_recv.at[z],
            b_send,
            b_recv,
            device_id={"sp": to},
            device_id_type=MESH,
        )

    def x_copy(slot, way):
        to = lax.rem(x + (1 if way == 0 else n_x - 1), n_x) * cores + core
        return pltpu.make_async_remote_copy(
            recv.at[slot, core, x],
            recv.at[slot, core, x],
            x_send.at[slot, way],
            x_recv.at[slot, way],
            device_id={"tp": to},
            device_id_type=MESH,
        )

    def x_arrival(slot, way):
        came = lax.rem(x + (n_x - 1 if way == 0 else 1), n_x)
        return pltpu.make_async_remote_copy(
            recv.at[slot, core, came],
            recv.at[slot, core, came],
            x_send.at[slot, way],
            x_recv.at[slot, way],
            device_id={"tp": partner},
            device_id_type=MESH,
        )

    def far_ref(slot, way, chip):
        return recv.at[slot, core, chip, pl.ds(way * piece, piece)]

    def far_copy(slot, way):
        came = lax.rem(x + (n_x - 1 if way == 0 else 1), n_x)
        to = lax.rem(x + (1 if way == 0 else n_x - 1), n_x) * cores + core
        return pltpu.make_async_remote_copy(
            far_ref(slot, way, came),
            far_ref(slot, way, came),
            far_send.at[slot, way],
            far_recv.at[slot, way],
            device_id={"tp": to},
            device_id_type=MESH,
        )

    def far_arrival(slot, way):
        came = lax.rem(x + 2, n_x)
        return pltpu.make_async_remote_copy(
            far_ref(slot, way, came),
            far_ref(slot, way, came),
            far_send.at[slot, way],
            far_recv.at[slot, way],
            device_id={"tp": partner},
            device_id_type=MESH,
        )

    def p_copy(slot):
        return pltpu.make_async_remote_copy(
            recv.at[slot, core], recv.at[slot, core], p_send.at[slot], p_recv.at[slot],
            device_id={"tp": partner}, device_id_type=MESH,
        )

    def p_arrival(slot):
        return pltpu.make_async_remote_copy(
            recv.at[slot, 1 - core], recv.at[slot, 1 - core], p_send.at[slot], p_recv.at[slot],
            device_id={"tp": partner}, device_id_type=MESH,
        )

    def part_copy():
        return pltpu.make_async_remote_copy(
            parts.at[rank], parts.at[rank], part_send, part_recv,
            device_id={"sp": at_rank(0)}, device_id_type=MESH,
        )

    def result_copy(r):
        return pltpu.make_async_remote_copy(
            result, result, result_send.at[r], result_recv, device_id={"sp": at_rank(r)}, device_id_type=MESH
        )

    for load in loads:
        load.wait()

    def send(q):
        z_copy(q).start()
        bias_copy(q).start()

    def answer(r, carry):
        first = jnp.where(r == 0, late, jnp.where(r <= late, r - 1, r))
        send(rank - jnp.where(rank > late, first, r))
        return carry

    lax.fori_loop(0, jnp.minimum(rank, FIRST), answer, 0)
    out_row, in_row = iota((4 * 2 * piece, 4 * 2 * piece), 0), iota((4 * 2 * piece, 4 * 2 * piece), 1)
    source = (
        lax.rem(out_row, 2) * (4 * piece)
        + lax.rem(lax.div(out_row, 2), 2) * (2 * piece)
        + lax.div(out_row, 4)
    )
    perm[...] = jnp.where(in_row == source, 1.0, 0.0).astype(BF16)
    later_mask[...] = jnp.where(iota((rows, rows), 0) > iota((rows, rows), 1), 1.0, 0.0).astype(BF16)

    gains = gain_v[...].astype(F32)
    for t in range(cores * n_x):
        gain_f[t] = jnp.concatenate(
            [gains[t * feat // LANES + j : t * feat // LANES + j + 1] for j in range(feat // LANES)], axis=1
        )
    queries = query_v[...].astype(F32)
    for s in range(seqs):
        query_f[s] = queries[s : s + 1]

    def project(piece_of, count):
        squares = jnp.zeros((count, feat), F32)
        for t in range(cores * n_x):
            value = piece_of(t).astype(F32)
            squares = squares + value * value
        inverse = lax.rsqrt(jnp.sum(squares, axis=1, keepdims=True) / width + norm_eps)
        for t in range(cores * n_x):
            value = piece_of(t).astype(F32) * inverse * gain_f[t]
            normed[pl.ds(0, count), pl.ds(t * feat, feat)] = value.astype(BF16)
        return jnp.dot(normed[pl.ds(0, count), :], weight_v[...], preferred_element_type=F32).astype(BF16)

    lane = iota((1, LANES), 1)

    def own_read(s, totals):
        projected = project(
            lambda t: tok_v[pl.ds(s * span, span), :, pl.ds(t * feat, feat)].reshape(rows, feat), rows
        )
        keys, values = projected[:, :columns], projected[:, columns:]
        head_row, head_lane = iota((8, columns), 0), lax.div(iota((8, columns), 1), head_size)
        spread = jnp.where(head_row == head_lane, query_f[s], 0.0).astype(BF16)
        logits = lax.dot_general(spread, keys, (((1,), (1,)), ((), ())), preferred_element_type=F32)
        terms = jnp.concatenate([bias_v[s].astype(F32), jnp.zeros((8 - heads, rows), F32)], axis=0)
        logits = logits * head_size ** (-0.5) + terms
        soft = jnp.log1p(jnp.exp(-jnp.abs(logits)))
        keep = jnp.minimum(-logits, 0.0) - soft
        take = jnp.minimum(logits, 0.0) - soft
        high = keep.astype(BF16).astype(F32)
        middle = (keep - high).astype(BF16).astype(F32)
        low = keep - high - middle
        split = jnp.concatenate([high, middle, low, jnp.zeros_like(low)], axis=0).astype(BF16)
        sums = jnp.dot(split, later_mask[...], preferred_element_type=F32)
        later = sums[0:8] + sums[8:16] + sums[16:24]
        weights = jnp.exp(take + later)
        high = weights.astype(BF16).astype(F32)
        split = jnp.concatenate([high, weights - high], axis=0).astype(BF16)
        mixed = jnp.dot(split, values, preferred_element_type=F32)
        mixed = mixed[0:8] + mixed[8:16]
        read = jnp.sum(jnp.where(head_row == head_lane, mixed, 0.0), axis=0, keepdims=True)
        parts[rank, :, pl.ds(pl.multiple_of(s * columns, columns), columns)] = read
        total = jnp.sum(keep, axis=1, keepdims=True)
        for h in range(heads):
            totals = totals + jnp.where(lane == s * heads + h, total[h : h + 1], 0.0)
        return totals

    own_tile = lax.div(lax.rem(z, span), per_tile)
    own_bias = pltpu.make_async_copy(
        bias.at[lax.div(z, span), :, pl.ds(pl.multiple_of(own_tile * LANES, LANES), LANES)],
        bias_recv.at[z],
        bias_own_sem,
    )
    own_bias.start()
    own.wait()

    parts[rank, :, pl.ds(blocks * LANES, LANES)] = lax.fori_loop(0, seqs, own_read, jnp.zeros((1, LANES), F32))

    @pl.when(rank > 0)
    def _():
        part_copy().start()

    lax.fori_loop(jnp.minimum(rank, FIRST), rank, answer, 0)

    def higher(q):
        @pl.when((q > rank) & (q < n))
        def _():
            pl.semaphore_wait(ready.at[q], 1)
            send(q)

    def step(k, carry):
        @pl.when(k >= P_LAG)
        def _():
            slot = k - P_LAG
            p_arrival(slot).wait_recv()
            projected = project(lambda t: recv[slot, t % cores, t // cores], 2 * piece)
            stacked = jnp.concatenate(
                [projected[:, j * LANES : (j + 1) * LANES] for j in range(2 * columns // LANES)], axis=0
            )
            placed = jnp.dot(perm[...], stacked, preferred_element_type=F32).astype(BF16)
            for half in range(2):
                q = 2 * slot + half
                at = at_rank(jnp.where(q <= rank, rank - q, q))
                cache_out[pl.ds(pl.multiple_of(at * 4 * piece, 4 * piece), 4 * piece)] = placed[
                    half * 4 * piece : (half + 1) * 4 * piece
                ]

        @pl.when((k >= FAR_LAG) & (k < steps + FAR_LAG))
        def _():
            slot = k - FAR_LAG
            for way in range(2):
                far_arrival(slot, way).wait_recv()
            p_copy(slot).start()

        @pl.when((k >= X_LAG) & (k < steps + X_LAG))
        def _():
            slot = k - X_LAG
            for way in range(2):
                x_arrival(slot, way).wait_recv()
                far_copy(slot, way).start()

        @pl.when((k >= Z_LAG) & (k < steps + Z_LAG))
        def _():
            slot = k - Z_LAG

            @pl.when(slot > 0)
            def _():
                z_arrival(2 * slot).wait_recv()

            z_arrival(2 * slot + 1).wait_recv()
            for way in range(2):
                x_copy(slot, way).start()

        higher(rank + 1 + 2 * k)
        higher(rank + 2 + 2 * k)
        return carry

    lax.fori_loop(0, steps + P_LAG, step, 0)

    @pl.when(rank == 0)
    def _():
        others = parts.at[pl.ds(1, n - 1)]
        pltpu.make_async_copy(others, others, part_recv).wait()
        by_position = [parts[late if j == 0 else j - 1 if j <= late else j] for j in range(n)]
        result[...] = stick(by_position, blocks, seqs)[0]

        def tell(r, carry):
            result_copy(r).start()
            return carry

        lax.fori_loop(1, n, tell, 0)

    own_bias.wait()
    others = pl.ds(0, n - 1)
    pltpu.make_async_copy(bias_recv.at[others], bias_recv.at[others], b_recv).wait()
    arrived = bias_recv[...].astype(F32)
    part = lax.rem(lax.rem(z, span), per_tile)
    chosen = arrived[:, :, 0:piece]
    for j in range(1, per_tile):
        chosen = jnp.where(part == j, arrived[:, :, j * piece : (j + 1) * piece], chosen)
    bias_out[...] = chosen.astype(BF16)

    @pl.when(rank > 0)
    def _():
        result_copy(0).wait_recv()

    for s in range(seqs):
        att_out[pl.ds(s, 1), :] = result[:, s * columns : (s + 1) * columns]

    pltpu.make_async_copy(bias_recv.at[others], bias_recv.at[others], b_send).wait()

    @pl.when(rank > 0)
    def _():
        part_copy().wait_send()

    @pl.when(rank == 0)
    def _():
        def told(r, carry):
            result_copy(r).wait_send()
            return carry

        lax.fori_loop(1, n, told, 0)

    def drain(slot, carry):
        for way in range(2):
            x_copy(slot, way).wait_send()
            far_copy(slot, way).wait_send()
        p_copy(slot).wait_send()

        @pl.when(slot > 0)
        def _():
            z_copy(2 * slot).wait_send()

        z_copy(2 * slot + 1).wait_send()
        return carry

    lax.fori_loop(0, steps, drain, 0)


def local(cores, tokens, norm_gain, key_weight, value_weight, break_bias, new_query):
    seqs, tok_rows, width = tokens.shape
    heads = break_bias.shape[2]
    columns = key_weight.shape[1]
    n = lax.axis_size("sp")
    n_tp = lax.axis_size("tp")
    n_x = n_tp // cores
    piece = tok_rows * seqs // n
    span = n // seqs
    steps = n // 2
    feat = width // n_tp
    shape = (n, cores, n_x, piece, seqs, heads, width, columns)
    dma = pltpu.SemaphoreType.DMA
    message = seqs * columns + LANES
    cache, bias_out, attended = pl.pallas_call(
        functools.partial(kernel, shape),
        out_shape=(
            jax.ShapeDtypeStruct((n * piece * 4, LANES), BF16),
            jax.ShapeDtypeStruct((n, heads, piece), BF16),
            jax.ShapeDtypeStruct((seqs, columns), F32),
        ),
        in_specs=[pl.BlockSpec(memory_space=pltpu.HBM)] * 6,
        out_specs=[pl.BlockSpec(memory_space=pltpu.VMEM)] * 3,
        scratch_shapes=[
            pltpu.VMEM((n, piece, width), BF16),
            pltpu.VMEM((width, 2 * columns), BF16),
            pltpu.VMEM((steps, cores, n_x, 2 * piece, feat), BF16),
            pltpu.VMEM((max(span, 2) * piece, width), BF16),
            pltpu.VMEM((seqs, heads, tok_rows), BF16),
            pltpu.VMEM((n, heads, LANES), BF16),
            pltpu.VMEM((seqs, columns), BF16),
            pltpu.VMEM((seqs, 1, columns), F32),
            pltpu.VMEM((width // LANES, LANES), BF16),
            pltpu.VMEM((n_tp, 1, feat), F32),
            pltpu.VMEM((8 * piece, 8 * piece), BF16),
            pltpu.VMEM((tok_rows, tok_rows), BF16),
            pltpu.VMEM((n, 1, message), F32),
            pltpu.VMEM((1, seqs * columns), F32),
            pltpu.SemaphoreType.REGULAR((n,)),
            dma((6,)),
            dma,
            dma,
            dma((n,)),
            dma((n,)),
            dma,
            dma,
            dma((steps, 2)),
            dma((steps, 2)),
            dma((steps, 2)),
            dma((steps, 2)),
            dma((steps,)),
            dma((steps,)),
            dma,
            dma,
            dma((n,)),
            dma,
        ],
        compiler_params=pltpu.CompilerParams(
            collective_id=0, has_side_effects=True, vmem_limit_bytes=48 * 1024 * 1024
        ),
    )(
        *(
            pltpu.with_memory_space_constraint(array, pltpu.HBM)
            for array in (
                tokens.reshape(n, piece, width),
                norm_gain.reshape(width // LANES, LANES),
                key_weight,
                value_weight,
                jnp.transpose(break_bias, (0, 2, 1)),
                new_query,
            )
        )
    )
    halves = columns // LANES
    paired = cache.reshape(n, piece, halves, 2, LANES)
    paired = jnp.transpose(paired, (0, 1, 3, 2, 4)).reshape(n, piece, 2, columns)
    return (paired[None], jnp.transpose(bias_out, (0, 2, 1))[None], attended)


def solution(mesh):
    return jax.shard_map(
        functools.partial(local, 2),
        mesh=mesh,
        in_specs=(
            P("grp", "sp", None),
            P(),
            P(None, "tp"),
            P(None, "tp"),
            P("grp", "sp", "tp"),
            P("grp", "tp"),
        ),
        out_specs=(
            P(("grp", "sp"), None, None, None, "tp"),
            P(("grp", "sp"), None, None, "tp"),
            P("grp", "tp"),
        ),
        check_vma=False,
    )
```
